256 devices in a mesh: rep: 2 (over z_hi), fs: 16 (over z_lo, y), tp: 8 (over x, core).
Axes of the slice: x: 4, y: 4, z: 8 (z_hi: 2, z_lo: 4; z = z_hi * 4 + z_lo), core: 2. Of those that a mesh axis runs over, the one named last changes fastest.
Arguments:
- stream: bfloat16 [16384, 2048], P(('rep', 'fs'), 'tp'), parts along dimension 0, may hold values from -6 to 6
- in_weight: bfloat16 [2048, 1024], P('fs', 'tp'), may hold values from -0.125 to 0.125
- pool_weight: bfloat16 [8, 128, 128], P('tp'), may hold values from -0.5 to 0.5
- pool_scale: bfloat16 [1024], P('tp'), may hold values from 0.099609375 to 1.8984375
- out_weight: bfloat16 [1024, 2048], P('tp', 'fs'), may hold values from -0.1875 to 0.1875
- mix_gain: bfloat16 [2048], replicated, may hold values from 0.099609375 to 1.8984375
- ffn_gain: bfloat16 [2048], replicated, may hold values from 0.099609375 to 1.8984375
- gate_weight: bfloat16 [2048, 5632], P('fs', 'tp'), may hold values from -0.125 to 0.125
- up_weight: bfloat16 [2048, 5632], P('fs', 'tp'), may hold values from -0.125 to 0.125
- down_weight: bfloat16 [5632, 2048], P('tp', 'fs'), may hold values from -0.078125 to 0.078125
Outputs:
- result: bfloat16 [16384, 2048], P(('rep', 'fs'), 'tp'), parts along dimension 0
The draws below stay inside these ranges and needn't reach their ends.
There are 2 independent parts, one for each index of `rep`. The reference program is written for one: setup_inputs(seed, part) draws one part's arguments, and reference() takes and returns one part's arrays. A program takes and returns all parts, laid end to end along the dimension named above; an argument that names none is the same for every part. Nothing has to cross between parts.
All inputs are finite; a program needn't handle non-finite values.
Results may differ from the reference program's by a relative error of at most 0.015.
Values may be sent and summed in bfloat16 or wider, within the bound.
A program may use at most 64 MiB of HBM per device.

```python
import jax
import jax.numpy as jnp
from jax import lax

D = 2048
GROUPS = 8
GROUP_DIM = 128
FF = 5632
SEQ = 128
POOL_CH = 1024
TOKENS = 8192
N_TP = 8


def block_scale(own_key, shape, split, least, high):
    factor_of, own = 1.0, jax.random.fold_in(own_key, 6)
    for axis_at, parts in split:
        steps = jnp.exp(jax.random.uniform(jax.random.fold_in(own, axis_at), (parts,), jnp.float32, least / len(split), high / len(split)))
        factor_of = factor_of * jnp.repeat(steps, shape[axis_at] // parts).reshape([-1 if axis == axis_at else 1 for axis in range(len(shape))])
    return factor_of


def bell_draw(rng, extent, width, bound, cuts=(), kind=jnp.bfloat16):
    array = width * jax.random.normal(rng, extent, jnp.float32)
    if cuts:
        array = array * block_scale(rng, extent, cuts, -0.22, 0.18)
    return jnp.clip(array, -bound, bound).astype(kind)


def setup_inputs(seed: int = 0, part: int = 0) -> dict:
    keys = jax.random.split(jax.random.key(seed), 11)
    part_keys = jax.random.split(jax.random.fold_in(keys[10], part), 11)
    return {
        "stream": bell_draw(part_keys[0], (TOKENS, D), 1.0, 6.0, ((0, 16), (1, 8))),
        "in_weight": bell_draw(keys[1], (D, POOL_CH), D ** -0.5, 0.125, ((0, 16), (1, 8))),
        "pool_weight": bell_draw(keys[2], (GROUPS, GROUP_DIM, GROUP_DIM), GROUP_DIM ** -0.5, 0.5, ((0, 8),)),
        "pool_scale": jnp.clip(1.0 + 0.18 * jax.random.normal(keys[3], (POOL_CH,), jnp.float32), 0.099609375, 1.8984375).astype(jnp.bfloat16),
        "out_weight": bell_draw(keys[4], (POOL_CH, D), POOL_CH ** -0.5, 0.1875, ((0, 8), (1, 16))),
        "mix_gain": jnp.clip(1.0 + 0.18 * jax.random.normal(keys[5], (D,), jnp.float32), 0.099609375, 1.8984375).astype(jnp.bfloat16),
        "ffn_gain": jnp.clip(1.0 + 0.18 * jax.random.normal(keys[6], (D,), jnp.float32), 0.099609375, 1.8984375).astype(jnp.bfloat16),
        "gate_weight": bell_draw(keys[7], (D, FF), D ** -0.5, 0.125, ((0, 16), (1, 8))),
        "up_weight": bell_draw(keys[8], (D, FF), D ** -0.5, 0.125, ((0, 16), (1, 8))),
        "down_weight": bell_draw(keys[9], (FF, D), FF ** -0.5, 0.078125, ((0, 8), (1, 16))),
    }


epsilon = 1e-06

def root_norm(values, gain_vec):
    widened = values.astype(jnp.float32)
    scaled = widened * lax.rsqrt(lax.optimization_barrier(jnp.mean(widened * widened, axis=-1, keepdims=True)) + epsilon)
    return (scaled * gain_vec.astype(jnp.float32)).astype(jnp.bfloat16)

def window_tables(first_group, group_count, seq_len, total_groups):
    group_ids = first_group + jnp.arange(group_count, dtype=jnp.int32)
    reaches = jnp.left_shift(jnp.int32(2), 4 * group_ids // total_groups)
    query_pos = jnp.arange(seq_len, dtype=jnp.int32)[:, None]
    earlier = jnp.arange(seq_len, dtype=jnp.int32)[None, :]
    inside = (earlier <= query_pos)[None] & (earlier[None] > query_pos[None] - reaches[:, None, None])
    counts = jnp.minimum(query_pos[:, 0][None, :] + 1, reaches[:, None]).astype(jnp.float32)
    return (inside, counts)

def block_sum(operand, weights):
    block_width = operand.shape[1] // N_TP
    running = jnp.zeros((operand.shape[0], weights.shape[1]), jnp.float32)
    for block_id in range(N_TP):
        product = jnp.dot(operand[:, block_id * block_width:(block_id + 1) * block_width], weights[block_id * block_width:(block_id + 1) * block_width], preferred_element_type=jnp.float32)
        rounded = lax.optimization_barrier(product.astype(jnp.bfloat16))
        running = running + rounded.astype(jnp.float32)
    return running

def reference(stream, in_weight, pool_weight, pool_scale, out_weight, mix_gain, ffn_gain, gate_weight, up_weight, down_weight):
    normed = root_norm(stream, mix_gain)
    pooled_in = jnp.dot(normed, in_weight, preferred_element_type=jnp.float32).astype(jnp.bfloat16)
    inside, counts = window_tables(0, GROUPS, SEQ, GROUPS)
    grouped = pooled_in.astype(jnp.float32).reshape(TOKENS // SEQ, SEQ, GROUPS, GROUP_DIM)
    window_sums = jnp.einsum('gts,nsgc->ntgc', inside.astype(jnp.float32), grouped, precision=lax.Precision.HIGHEST)
    contrast = (window_sums / counts.T[None, :, :, None] - grouped).astype(jnp.bfloat16)
    mixed_out = jnp.einsum('ntgc,gcd->ntgd', contrast.astype(jnp.float32), pool_weight.astype(jnp.float32))
    group_out = (mixed_out.reshape(TOKENS, POOL_CH) * pool_scale.astype(jnp.float32)).astype(jnp.bfloat16)
    mixer_sum = block_sum(group_out, out_weight)
    middle = (stream.astype(jnp.float32) + mixer_sum).astype(jnp.bfloat16)
    normed_ffn = root_norm(middle, ffn_gain)
    gate_acts = jnp.dot(normed_ffn, gate_weight, preferred_element_type=jnp.float32)
    up_acts = jnp.dot(normed_ffn, up_weight, preferred_element_type=jnp.float32)
    hidden = (jax.nn.silu(gate_acts) * up_acts).astype(jnp.bfloat16)
    ffn_sum = block_sum(hidden, down_weight)
    return (middle.astype(jnp.float32) + ffn_sum).astype(jnp.bfloat16)
```

```python
import jax
import jax.numpy as jnp
from jax import lax
from jax.experimental import pallas as pl
from jax.experimental.pallas import tpu as pltpu
from jax.sharding import Mesh
from jax.sharding import PartitionSpec as P

SEQ = 128
RING = 4
EPS = 1e-06
F32, BF16 = jnp.float32, jnp.bfloat16


class Place:
    def __init__(self):
        self.rep, self.z, self.y = (lax.axis_index(a) for a in ("rep", "fs_0", "fs_1"))
        self.x, self.core = lax.axis_index("x"), lax.axis_index("core")

    def to(self, axis, step):
        if axis == "core":
            return {"core": 1 - self.core}
        if axis == "z":
            deep = (self.rep * RING + self.z + step + 2 * RING) % (2 * RING)
            return {"rep": deep // RING, "fs_0": deep % RING}
        index = {"x": self.x, "y": self.y}[axis]
        return {{"x": "x", "y": "fs_1"}[axis]: (index + step + RING) % RING}


class Sends:
    def __init__(self, send_sems, recv_sems):
        self.send_sems, self.recv_sems, self.open = send_sems, recv_sems, []

    def send(self, k, src, dst, device):
        copy = pltpu.make_async_remote_copy(
            src_ref=src,
            dst_ref=dst,
            send_sem=self.send_sems.at[k],
            recv_sem=self.recv_sems.at[k],
            device_id=device,
            device_id_type=pl.DeviceIdType.MESH,
        )
        copy.start()
        self.open.append(copy)

    def arrived(self, k, ref):
        pltpu.make_async_copy(ref, ref, self.recv_sems.at[k]).wait()

    def drain(self):
        for copy in self.open:
            copy.wait_send()


class Gather:
    def __init__(self, place, buf, send_sems, recv_sems):
        self.place, self.buf = place, buf
        self.net = Sends(send_sems, recv_sems)
        half = buf.shape[2] // 2
        self.flows = (("y", "z", 0, half, 0), ("z", "y", half, half, 10))

    def block(self, axis, step, first, rows):
        z, y = self.place.z, self.place.y
        z, y = ((z + step) % RING, y) if axis == "z" else (z, (y + step) % RING)
        return self.buf.at[z, y, pl.ds(first, rows), :]

    def plane(self, axis, step, side, first, rows):
        two = pl.ds(2 * side, 2)
        if axis == "z":
            return self.buf.at[(self.place.z + step) % RING, two, pl.ds(first, rows), :]
        return self.buf.at[two, (self.place.y + step) % RING, pl.ds(first, rows), :]

    def p1_own(self):
        for axis, _, first, rows, k in self.flows:
            own = self.block(axis, 0, first, rows)
            self.net.send(k, own, own, self.place.to(axis, 1))
            self.net.send(k + 1, own, own, self.place.to(axis, -1))

    def p1_forward(self):
        for axis, _, first, rows, k in self.flows:
            half = rows // 2
            self.net.arrived(k, self.block(axis, 3, first, rows))
            low = self.block(axis, 3, first, half)
            self.net.send(k + 2, low, low, self.place.to(axis, 1))
            self.net.arrived(k + 1, self.block(axis, 1, first, rows))
            high = self.block(axis, 1, first + half, half)
            self.net.send(k + 3, high, high, self.place.to(axis, -1))

    def p2_own(self):
        for before, axis, first, rows, k in self.flows:
            half = rows // 2
            self.net.arrived(k + 2, self.block(before, 2, first, half))
            self.net.arrived(k + 3, self.block(before, 2, first + half, half))
            low, high = (self.plane(axis, 0, side, first, rows) for side in (0, 1))
            self.net.send(k + 4, low, low, self.place.to(axis, 1))
            self.net.send(k + 7, high, high, self.place.to(axis, -1))
            self.net.send(k + 5, high, high, self.place.to(axis, 1))
            self.net.send(k + 6, low, low, self.place.to(axis, -1))

    def p2_forward(self):
        for _, axis, first, rows, k in self.flows:
            low, high = self.plane(axis, 3, 0, first, rows), self.plane(axis, 1, 1, first, rows)
            self.net.arrived(k + 4, low)
            self.net.send(k + 8, low, low, self.place.to(axis, 1))
            self.net.arrived(k + 7, high)
            self.net.send(k + 9, high, high, self.place.to(axis, -1))

    def finish(self):
        for _, axis, first, rows, k in self.flows:
            self.net.arrived(k + 5, self.plane(axis, 3, 1, first, rows))
            self.net.arrived(k + 6, self.plane(axis, 1, 0, first, rows))
            self.net.arrived(k + 8, self.plane(axis, 2, 0, first, rows))
            self.net.arrived(k + 9, self.plane(axis, 2, 1, first, rows))


class Spread:
    def __init__(self, place, buf, send_sems, recv_sems):
        self.place, self.buf = place, buf
        self.net = Sends(send_sems, recv_sems)
        self.half = buf.shape[1] // 2

    def index(self, step, other=False):
        core = 1 - self.place.core if other else self.place.core
        return 2 * ((self.place.x + step) % RING) + core

    def part(self, step, side):
        return self.buf.at[self.index(step), pl.ds(side * self.half, self.half), :]

    def to_core(self, k, step):
        block = self.buf.at[self.index(step)]
        self.net.send(k, block, block, self.place.to("core", 0))

    def start(self):
        up, down = self.place.to("x", 1), self.place.to("x", -1)
        low, high = self.part(0, 0), self.part(0, 1)
        self.net.send(0, low, low, up)
        self.net.send(2, high, high, down)
        self.net.send(1, high, high, up)
        self.net.send(3, low, low, down)
        self.to_core(6, 0)

    def forward(self):
        low, high = self.part(3, 0), self.part(1, 1)
        self.net.arrived(0, low)
        self.net.send(4, low, low, self.place.to("x", 1))
        self.net.arrived(2, high)
        self.net.send(5, high, high, self.place.to("x", -1))

    def near(self):
        self.net.arrived(1, self.part(3, 1))
        self.to_core(7, 3)
        self.net.arrived(3, self.part(1, 0))
        self.to_core(8, 1)

    def far(self):
        self.net.arrived(4, self.part(2, 0))
        self.net.arrived(5, self.part(2, 1))
        self.to_core(9, 2)

    def from_core(self, k, step):
        self.net.arrived(k, self.buf.at[self.index(step, other=True)])


def kernel(
    stream, w_in, pool_w, pool_s, w_out, mix_gain, ffn_gain, w_gate, w_up, w_down, out,
    mixer, pair_a, pair_b, down, blocks_a, blocks_b, scaled, squares, rates, group_out, hidden,
    pair_out, pair_in, sums, last, combined, landed, gs, gr, xs, xr,
):
    place = Place()
    x, core, y, z = place.x, place.core, place.y, place.z
    mine = 2 * x + core
    tokens = stream.shape[0]
    half = tokens // 2

    barrier = pltpu.get_barrier_semaphore()
    neighbours = [place.to(a, s) for a in "xyz" for s in (1, -1)] + [place.to("core", 0)]
    for device in neighbours:
        pl.semaphore_signal(barrier, inc=1, device_id=device, device_id_type=pl.DeviceIdType.MESH)

    mixer[z, y, 0:128, :] = w_in[...]
    mixer[z, y, 128:256, :] = w_out[...]
    blocks_a[mine] = stream[...]
    for tile in range(5):
        buf, at = (pair_a, tile) if tile < 3 else (pair_b, tile - 3)
        lanes = slice(128 * tile, 128 * tile + 128)
        buf[z, y, :, 256 * at : 256 * at + 128] = w_gate[:, lanes]
        buf[z, y, :, 256 * at + 128 : 256 * at + 256] = w_up[:, lanes]
    pair_b[z, y, :, 512:640] = jnp.concatenate([w_gate[:, 640:704], w_up[:, 640:704]], axis=1)
    down[z, y] = w_down[...]

    pl.semaphore_wait(barrier, len(neighbours))

    gathers = [
        Gather(place, buf, gs.at[i], gr.at[i]) for i, buf in enumerate((mixer, pair_a, pair_b, down))
    ]
    g_mix, g_a, g_b, g_down = gathers
    s_in = Spread(place, blocks_a, xs.at[0], xr.at[0])
    s_mid = Spread(place, blocks_b, xs.at[1], xr.at[1])

    def take(buf, gain_ref, index, first=False):
        lanes = pl.ds(pl.multiple_of(index * 256, 256), 256)
        gain = gain_ref[:, lanes].astype(F32)

        def some(i, carry):
            rows = pl.ds(pl.multiple_of(i * 64, 64), 64)
            value = buf[index, rows, :].astype(F32)
            scaled[rows, lanes] = (value * gain).astype(BF16)
            square = value * value
            square = square[:, :128] + square[:, 128:]
            squares[rows, :] = square if first else squares[rows, :] + square
            return carry

        lax.fori_loop(0, tokens // 64, some, 0)

    def row_rates():
        total = jnp.sum(squares[...], axis=1, keepdims=True)
        rates[...] = jnp.broadcast_to(lax.rsqrt(total * (1.0 / 2048.0) + EPS), (tokens, 128))

    def rows_of(side):
        return pl.ds(side * half, half)

    class Summed:
        def __init__(self, which):
            self.net = Sends(xs.at[which], xr.at[which])
            self.out, self.into = pair_out.at[which], pair_in.at[which]
            self.sums, self.last = sums.at[which], last
            self.combined, self.landed = combined.at[which], landed.at[which]

        def pair(self, product):
            for j, step in enumerate((2, 1, 3, 0)):
                for side in (0, 1):
                    self.out[j, rows_of(side), :] = product((x + step) % RING, 1 - core, side).astype(BF16)
                self.net.send(10 + j, self.out.at[j], self.into.at[j], place.to("core", 0))

        def start(self, product):
            plus, minus = place.to("x", 1), place.to("x", -1)
            sums, landed = self.sums, self.landed
            for j, step in enumerate((2, 1, 3, 0)):
                parts = [product((x + step) % RING, core, side) for side in (0, 1)]
                self.net.arrived(10 + j, self.into.at[j])
                for side in (0, 1):
                    total = parts[side] + self.into[j, rows_of(side), :].astype(F32)
                    if j == 3:
                        self.last[rows_of(side), :] = total
                    else:
                        sums[j, rows_of(side), :] = total.astype(BF16)
                if j == 0:
                    self.net.send(14, sums.at[0, rows_of(0)], landed.at[0], plus)
                    self.net.send(15, sums.at[0, rows_of(1)], landed.at[1], minus)
                if j == 1:
                    self.net.send(16, sums.at[1, rows_of(1)], landed.at[2], plus)
                if j == 2:
                    self.net.send(17, sums.at[2, rows_of(0)], landed.at[3], minus)

        def forward(self):
            plus, minus = place.to("x", 1), place.to("x", -1)
            for side, device in ((0, plus), (1, minus)):
                self.net.arrived(14 + side, self.landed.at[side])
                total = self.sums[1 + side, rows_of(side), :].astype(F32) + self.landed[side].astype(F32)
                self.combined[side] = total.astype(BF16)
                self.net.send(18 + side, self.combined.at[side], self.landed.at[4 + side], device)

        def result(self, base, store):
            self.net.arrived(16, self.landed.at[2])
            self.net.arrived(17, self.landed.at[3])
            for side in (0, 1):
                self.net.arrived(18 + side, self.landed.at[4 + side])
                total = (
                    self.last[rows_of(side), :]
                    + self.landed[3 - side].astype(F32)
                    + self.landed[4 + side].astype(F32)
                )
                store(side, (base(side).astype(F32) + total).astype(BF16))

    r_mix, r_ffn = Summed(0), Summed(1)

    g_mix.p1_own()
    s_in.start()
    g_a.p1_own()
    g_mix.p1_forward()
    g_b.p1_own()
    take(blocks_a, mix_gain, mine, first=True)
    g_mix.p2_own()
    g_down.p1_own()
    s_in.from_core(6, 0)
    take(blocks_a, mix_gain, s_in.index(0, other=True))
    s_in.forward()
    g_mix.p2_forward()
    g_a.p1_forward()
    g_b.p1_forward()
    g_down.p1_forward()
    s_in.near()
    for step in (3, 1):
        take(blocks_a, mix_gain, s_in.index(step))
    s_in.far()
    take(blocks_a, mix_gain, s_in.index(2))
    for k, step in ((7, 3), (8, 1), (9, 2)):
        s_in.from_core(k, step)
        take(blocks_a, mix_gain, s_in.index(step, other=True))
    row_rates()
    g_a.p2_own()
    g_mix.finish()

    pooled = jnp.dot(
        scaled[...], mixer[:, :, 0:128, :].reshape(2048, 128), preferred_element_type=F32
    )
    pooled = (pooled * rates[...]).astype(BF16)
    reach = jnp.where(x == 0, 2, jnp.where(x == 1, 4, jnp.where(x == 2, 8, 16)))
    query = lax.broadcasted_iota(jnp.int32, (SEQ, SEQ), 0)
    earlier = lax.broadcasted_iota(jnp.int32, (SEQ, SEQ), 1)
    inside = jnp.where((earlier <= query) & (earlier > query - reach), 1.0, 0.0).astype(BF16)
    counts = jnp.minimum(query + 1, reach).astype(F32)
    scale = pool_s[...].astype(F32)
    for s in range(tokens // SEQ):
        rows = slice(s * SEQ, s * SEQ + SEQ)
        part = pooled[rows]
        window = jnp.dot(inside, part, preferred_element_type=F32)
        contrast = (window / counts - part.astype(F32)).astype(BF16)
        mixed = jnp.dot(contrast, pool_w[0], preferred_element_type=F32)
        group_out[rows, :] = (mixed * scale).astype(BF16)

    def mix_product(owner_x, owner_core, side):
        pair = mixer[owner_x, pl.ds(2 * owner_core, 2), 128:256, :]
        weights = jnp.concatenate([pair[0], pair[1]], axis=1)
        return jnp.dot(group_out[rows_of(side), :], weights, preferred_element_type=F32)

    r_mix.pair(mix_product)
    g_b.p2_own()
    r_mix.start(mix_product)
    r_mix.forward()
    g_a.p2_forward()

    def store_middle(side, value):
        blocks_b[mine, rows_of(side), :] = value

    r_mix.result(lambda side: stream[rows_of(side), :], store_middle)
    s_mid.start()
    g_b.p2_forward()
    g_down.p2_own()
    take(blocks_b, ffn_gain, mine, first=True)
    s_mid.from_core(6, 0)
    take(blocks_b, ffn_gain, s_mid.index(0, other=True))
    s_mid.forward()
    s_mid.near()
    for step in (3, 1):
        take(blocks_b, ffn_gain, s_mid.index(step))
    s_mid.far()
    take(blocks_b, ffn_gain, s_mid.index(2))
    for k, step in ((7, 3), (8, 1), (9, 2)):
        s_mid.from_core(k, step)
        take(blocks_b, ffn_gain, s_mid.index(step, other=True))
    row_rates()

    def units(buf, at, width, column):
        weights = buf[:, :, :, at : at + 2 * width].reshape(2048, 2 * width)

        def some(i, carry):
            rows = pl.ds(pl.multiple_of(i * 256, 256), 256)
            acts = jnp.dot(scaled[rows, :], weights, preferred_element_type=F32)
            rate = rates[rows, 0:width]
            gate, up = acts[:, :width] * rate, acts[:, width:] * rate
            hidden[rows, column : column + width] = (gate / (1.0 + jnp.exp(-gate)) * up).astype(BF16)
            return carry

        lax.fori_loop(0, tokens // 256, some, 0)

    g_a.finish()
    for chunk in range(3):
        units(pair_a, 256 * chunk, 128, 128 * chunk)
    g_down.p2_forward()
    g_b.finish()
    for chunk in range(2):
        units(pair_b, 256 * chunk, 128, 384 + 128 * chunk)
    units(pair_b, 512, 64, 640)
    g_down.finish()

    def ffn_product(owner_x, owner_core, side):
        pair = down[owner_x, pl.ds(2 * owner_core, 2)]
        weights = jnp.concatenate([pair[0], pair[1]], axis=1)
        return jnp.dot(hidden[rows_of(side), :], weights, preferred_element_type=F32)

    r_ffn.pair(ffn_product)
    r_ffn.start(ffn_product)
    r_ffn.forward()

    def store_result(side, value):
        out[rows_of(side), :] = value

    r_ffn.result(lambda side: blocks_b[mine, rows_of(side), :], store_result)

    for net in [g.net for g in gathers] + [s_in.net, s_mid.net, r_mix.net, r_ffn.net]:
        net.drain()


def on_device(stream, in_weight, pool_weight, pool_scale, out_weight, mix_gain, ffn_gain, gate_weight, up_weight, down_weight):
    tokens = stream.shape[0]
    half = tokens // 2
    return pl.pallas_call(
        kernel,
        out_shape=jax.ShapeDtypeStruct(stream.shape, BF16),
        in_specs=[pl.BlockSpec(memory_space=pltpu.VMEM)] * 10,
        out_specs=pl.BlockSpec(memory_space=pltpu.VMEM),
        scratch_shapes=[
            pltpu.VMEM((4, 4, 256, 128), BF16),
            pltpu.VMEM((4, 4, 128, 768), BF16),
            pltpu.VMEM((4, 4, 128, 640), BF16),
            pltpu.VMEM((4, 4, 704, 128), BF16),
            pltpu.VMEM((8, tokens, 256), BF16),
            pltpu.VMEM((8, tokens, 256), BF16),
            pltpu.VMEM((tokens, 2048), BF16),
            pltpu.VMEM((tokens, 128), F32),
            pltpu.VMEM((tokens, 128), F32),
            pltpu.VMEM((tokens, 128), BF16),
            pltpu.VMEM((tokens, 704), BF16),
            pltpu.VMEM((2, 4, tokens, 256), BF16),
            pltpu.VMEM((2, 4, tokens, 256), BF16),
            pltpu.VMEM((2, 3, tokens, 256), BF16),
            pltpu.VMEM((tokens, 256), F32),
            pltpu.VMEM((2, 2, half, 256), BF16),
            pltpu.VMEM((2, 6, half, 256), BF16),
            pltpu.SemaphoreType.DMA((4, 20)),
            pltpu.SemaphoreType.DMA((4, 20)),
            pltpu.SemaphoreType.DMA((2, 20)),
            pltpu.SemaphoreType.DMA((2, 20)),
        ],
        compiler_params=pltpu.CompilerParams(
            collective_id=0, has_side_effects=True, vmem_limit_bytes=60 * 1024 * 1024
        ),
    )(
        stream, in_weight, pool_weight, pool_scale.reshape(1, -1), out_weight,
        mix_gain.reshape(1, -1), ffn_gain.reshape(1, -1), gate_weight, up_weight, down_weight,
    )


def solution(mesh):
    finer = Mesh(
        mesh.devices.reshape(mesh.shape["rep"], RING, RING, RING, 2),
        ("rep", "fs_0", "fs_1", "x", "core"),
    )
    fs, tp = ("fs_0", "fs_1"), ("x", "core")
    rows = ("rep", *fs)
    return jax.shard_map(
        on_device,
        mesh=finer,
        in_specs=(
            P(rows, tp), P(fs, tp), P(tp, None, None), P(tp), P(tp, fs),
            P(), P(), P(fs, tp), P(fs, tp), P(tp, fs),
        ),
        out_specs=P(rows, tp),
        check_vma=False,
    )
```

```python
import jax
import jax.numpy as jnp
from jax import lax
from jax.experimental import pallas as pl
from jax.experimental.pallas import tpu as pltpu
from jax.sharding import Mesh
from jax.sharding import PartitionSpec as P

SEQ = 128
RING = 4
EPS = 1e-06
F32, BF16 = jnp.float32, jnp.bfloat16


class Place:
    def __init__(self):
        self.rep, self.z, self.y = (lax.axis_index(a) for a in ("rep", "fs_0", "fs_1"))
        self.x, self.core = lax.axis_index("x"), lax.axis_index("core")

    def to(self, axis, step):
        if axis == "core":
            return {"core": 1 - self.core}
        if axis == "z":
            deep = (self.rep * RING + self.z + step + 2 * RING) % (2 * RING)
            return {"rep": deep // RING, "fs_0": deep % RING}
        index = {"x": self.x, "y": self.y}[axis]
        return {{"x": "x", "y": "fs_1"}[axis]: (index + step + RING) % RING}


class Sends:
    def __init__(self, send_sems, recv_sems):
        self.send_sems, self.recv_sems, self.open = send_sems, recv_sems, []

    def send(self, k, src, dst, device):
        copy = pltpu.make_async_remote_copy(
            src_ref=src,
            dst_ref=dst,
            send_sem=self.send_sems.at[k],
            recv_sem=self.recv_sems.at[k],
            device_id=device,
            device_id_type=pl.DeviceIdType.MESH,
        )
        copy.start()
        self.open.append(copy)

    def arrived(self, k, ref):
        pltpu.make_async_copy(ref, ref, self.recv_sems.at[k]).wait()

    def drain(self):
        for copy in self.open:
            copy.wait_send()


class Gather:
    def __init__(self, place, buf, send_sems, recv_sems):
        self.place, self.buf = place, buf
        self.net = Sends(send_sems, recv_sems)
        half = buf.shape[2] // 2
        self.flows = (("y", "z", 0, half, 0), ("z", "y", half, half, 10))

    def block(self, axis, step, first, rows):
        z, y = self.place.z, self.place.y
        z, y = ((z + step) % RING, y) if axis == "z" else (z, (y + step) % RING)
        return self.buf.at[z, y, pl.ds(first, rows), :]

    def plane(self, axis, step, side, first, rows):
        two = pl.ds(2 * side, 2)
        if axis == "z":
            return self.buf.at[(self.place.z + step) % RING, two, pl.ds(first, rows), :]
        return self.buf.at[two, (self.place.y + step) % RING, pl.ds(first, rows), :]

    def p1_own(self):
        for axis, _, first, rows, k in self.flows:
            own = self.block(axis, 0, first, rows)
            self.net.send(k, own, own, self.place.to(axis, 1))
            self.net.send(k + 1, own, own, self.place.to(axis, -1))

    def p1_forward(self):
        for axis, _, first, rows, k in self.flows:
            half = rows // 2
            self.net.arrived(k, self.block(axis, 3, first, rows))
            low = self.block(axis, 3, first, half)
            self.net.send(k + 2, low, low, self.place.to(axis, 1))
            self.net.arrived(k + 1, self.block(axis, 1, first, rows))
            high = self.block(axis, 1, first + half, half)
            self.net.send(k + 3, high, high, self.place.to(axis, -1))

    def p2_own(self):
        for before, axis, first, rows, k in self.flows:
            half = rows // 2
            self.net.arrived(k + 2, self.block(before, 2, first, half))
            self.net.arrived(k + 3, self.block(before, 2, first + half, half))
            low, high = (self.plane(axis, 0, side, first, rows) for side in (0, 1))
            self.net.send(k + 4, low, low, self.place.to(axis, 1))
            self.net.send(k + 7, high, high, self.place.to(axis, -1))
            self.net.send(k + 5, high, high, self.place.to(axis, 1))
            self.net.send(k + 6, low, low, self.place.to(axis, -1))

    def p2_forward(self):
        for _, axis, first, rows, k in self.flows:
            low, high = self.plane(axis, 3, 0, first, rows), self.plane(axis, 1, 1, first, rows)
            self.net.arrived(k + 4, low)
            self.net.send(k + 8, low, low, self.place.to(axis, 1))
            self.net.arrived(k + 7, high)
            self.net.send(k + 9, high, high, self.place.to(axis, -1))

    def finish(self):
        for _, axis, first, rows, k in self.flows:
            self.net.arrived(k + 5, self.plane(axis, 3, 1, first, rows))
            self.net.arrived(k + 6, self.plane(axis, 1, 0, first, rows))
            self.net.arrived(k + 8, self.plane(axis, 2, 0, first, rows))
            self.net.arrived(k + 9, self.plane(axis, 2, 1, first, rows))


class Spread:
    def __init__(self, place, buf, send_sems, recv_sems):
        self.place, self.buf = place, buf
        self.net = Sends(send_sems, recv_sems)
        self.half = buf.shape[1] // 2

    def index(self, step, other=False):
        core = 1 - self.place.core if other else self.place.core
        return 2 * ((self.place.x + step) % RING) + core

    def part(self, step, side):
        return self.buf.at[self.index(step), pl.ds(side * self.half, self.half), :]

    def to_core(self, k, step):
        block = self.buf.at[self.index(step)]
        self.net.send(k, block, block, self.place.to("core", 0))

    def start(self):
        up, down = self.place.to("x", 1), self.place.to("x", -1)
        low, high = self.part(0, 0), self.part(0, 1)
        self.net.send(0, low, low, up)
        self.net.send(2, high, high, down)
        self.net.send(1, high, high, up)
        self.net.send(3, low, low, down)
        self.to_core(6, 0)

    def forward(self):
        low, high = self.part(3, 0), self.part(1, 1)
        self.net.arrived(0, low)
        self.net.send(4, low, low, self.place.to("x", 1))
        self.net.arrived(2, high)
        self.net.send(5, high, high, self.place.to("x", -1))

    def near(self):
        self.net.arrived(1, self.part(3, 1))
        self.to_core(7, 3)
        self.net.arrived(3, self.part(1, 0))
        self.to_core(8, 1)

    def far(self):
        self.net.arrived(4, self.part(2, 0))
        self.net.arrived(5, self.part(2, 1))
        self.to_core(9, 2)

    def from_core(self, k, step):
        self.net.arrived(k, self.buf.at[self.index(step, other=True)])


def kernel(
    stream, w_in, pool_w_in, pool_s_in, w_out, mix_gain_in, ffn_gain_in, w_gate, w_up, w_down, out,
    gains, mix_gain, ffn_gain, gate_in, up_in, pool_w, pool_s, mixer, pair_a, pair_b, down, blocks_a, blocks_b, scaled, squares, rates, group_out, hidden,
    pair_out, pair_in, sums, last, combined, landed, fetched, gs, gr, xs, xr,
):
    place = Place()
    x, core, y, z = place.x, place.core, place.y, place.z
    mine = 2 * x + core
    tokens = stream.shape[0]
    half = tokens // 2

    barrier = pltpu.get_barrier_semaphore()
    neighbours = [place.to(a, s) for a in "xyz" for s in (1, -1)] + [place.to("core", 0)]
    for device in neighbours:
        pl.semaphore_signal(barrier, inc=1, device_id=device, device_id_type=pl.DeviceIdType.MESH)

    fetches = [
        pltpu.make_async_copy(src, dst, fetched.at[i])
        for i, (src, dst) in enumerate((
            (stream, blocks_a.at[mine]),
            (w_in, mixer.at[z, y, pl.ds(0, 128), :]),
            (w_out, mixer.at[z, y, pl.ds(128, 128), :]),
            (w_gate, gate_in),
            (w_up, up_in),
            (w_down, down.at[z, y]),
            (mix_gain_in, gains.at[0]),
            (ffn_gain_in, gains.at[1]),
            (pool_w_in, pool_w),
            (pool_s_in, pool_s),
        ))
    ]
    for fetch in fetches:
        fetch.start()
    pl.semaphore_wait(barrier, len(neighbours))

    gathers = [
        Gather(place, buf, gs.at[i], gr.at[i]) for i, buf in enumerate((mixer, pair_a, pair_b, down))
    ]
    g_mix, g_a, g_b, g_down = gathers
    s_in = Spread(place, blocks_a, xs.at[0], xr.at[0])
    s_mid = Spread(place, blocks_b, xs.at[1], xr.at[1])

    def take(buf, gain_ref, index, first=False):
        lanes = pl.ds(pl.multiple_of(index * 256, 256), 256)
        gain = jnp.concatenate([gain_ref[pl.ds(2 * index + i, 1), :] for i in (0, 1)], axis=1)

        def some(i, carry):
            rows = pl.ds(pl.multiple_of(i * 64, 64), 64)
            value = buf[index, rows, :].astype(F32)
            scaled[rows, lanes] = (value * gain).astype(BF16)
            square = value * value
            square = square[:, :128] + square[:, 128:]
            squares[rows, :] = square if first else squares[rows, :] + square
            return carry

        lax.fori_loop(0, tokens // 64, some, 0)

    def row_rates():
        total = jnp.sum(squares[...], axis=1, keepdims=True)
        rates[...] = jnp.broadcast_to(lax.rsqrt(total * (1.0 / 2048.0) + EPS), (tokens, 128))

    def rows_of(side):
        return pl.ds(side * half, half)

    class Summed:
        def __init__(self, which):
            self.net = Sends(xs.at[which], xr.at[which])
            self.out, self.into = pair_out.at[which], pair_in.at[which]
            self.sums, self.last = sums.at[which], last
            self.combined, self.landed = combined.at[which], landed.at[which]

        def pair(self, product):
            for j, step in enumerate((2, 1, 3, 0)):
                for side in (0, 1):
                    self.out[j, rows_of(side), :] = product((x + step) % RING, 1 - core, side).astype(BF16)
                self.net.send(10 + j, self.out.at[j], self.into.at[j], place.to("core", 0))

        def start(self, product):
            plus, minus = place.to("x", 1), place.to("x", -1)
            sums, landed = self.sums, self.landed
            for j, step in enumerate((2, 1, 3, 0)):
                parts = [product((x + step) % RING, core, side) for side in (0, 1)]
                self.net.arrived(10 + j, self.into.at[j])
                for side in (0, 1):
                    total = parts[side] + self.into[j, rows_of(side), :].astype(F32)
                    if j == 3:
                        self.last[rows_of(side), :] = total
                    else:
                        sums[j, rows_of(side), :] = total.astype(BF16)
                if j == 0:
                    self.net.send(14, sums.at[0, rows_of(0)], landed.at[0], plus)
                    self.net.send(15, sums.at[0, rows_of(1)], landed.at[1], minus)
                if j == 1:
                    self.net.send(16, sums.at[1, rows_of(1)], landed.at[2], plus)
                if j == 2:
                    self.net.send(17, sums.at[2, rows_of(0)], landed.at[3], minus)

        def forward(self):
            plus, minus = place.to("x", 1), place.to("x", -1)
            for side, device in ((0, plus), (1, minus)):
                self.net.arrived(14 + side, self.landed.at[side])
                total = self.sums[1 + side, rows_of(side), :].astype(F32) + self.landed[side].astype(F32)
                self.combined[side] = total.astype(BF16)
                self.net.send(18 + side, self.combined.at[side], self.landed.at[4 + side], device)

        def result(self, base, store):
            self.net.arrived(16, self.landed.at[2])
            self.net.arrived(17, self.landed.at[3])
            for side in (0, 1):
                self.net.arrived(18 + side, self.landed.at[4 + side])
                total = (
                    self.last[rows_of(side), :]
                    + self.landed[3 - side].astype(F32)
                    + self.landed[4 + side].astype(F32)
                )
                store(side, (base(side).astype(F32) + total).astype(BF16))

    r_mix, r_ffn = Summed(0), Summed(1)

    fetches[0].wait()
    s_in.start()
    fetches[1].wait()
    fetches[2].wait()
    g_mix.p1_own()
    fetches[3].wait()
    fetches[4].wait()
    for tile in range(5):
        buf, at = (pair_a, tile) if tile < 3 else (pair_b, tile - 3)
        some = slice(128 * tile, 128 * tile + 128)
        buf[z, y, :, 256 * at : 256 * at + 128] = gate_in[some, :].T
        buf[z, y, :, 256 * at + 128 : 256 * at + 256] = up_in[some, :].T
    pair_b[z, y, :, 512:640] = jnp.concatenate([gate_in[640:704, :], up_in[640:704, :]], axis=0).T
    for fetch in fetches[5:]:
        fetch.wait()
    mix_gain[...] = gains[0].astype(F32)
    ffn_gain[...] = gains[1].astype(F32)
    g_a.p1_own()
    g_mix.p1_forward()
    g_b.p1_own()
    take(blocks_a, mix_gain, mine, first=True)
    g_mix.p2_own()
    g_down.p1_own()
    s_in.from_core(6, 0)
    take(blocks_a, mix_gain, s_in.index(0, other=True))
    s_in.forward()
    g_mix.p2_forward()
    g_a.p1_forward()
    g_b.p1_forward()
    g_down.p1_forward()
    s_in.near()
    for step in (3, 1):
        take(blocks_a, mix_gain, s_in.index(step))
    s_in.far()
    take(blocks_a, mix_gain, s_in.index(2))
    for k, step in ((7, 3), (8, 1), (9, 2)):
        s_in.from_core(k, step)
        take(blocks_a, mix_gain, s_in.index(step, other=True))
    row_rates()
    g_a.p2_own()
    g_mix.finish()

    pooled = jnp.dot(
        scaled[...], mixer[:, :, 0:128, :].reshape(2048, 128), preferred_element_type=F32
    )
    pooled = (pooled * rates[...]).astype(BF16)
    reach = jnp.where(x == 0, 2, jnp.where(x == 1, 4, jnp.where(x == 2, 8, 16)))
    query = lax.broadcasted_iota(jnp.int32, (SEQ, SEQ), 0)
    earlier = lax.broadcasted_iota(jnp.int32, (SEQ, SEQ), 1)
    inside = jnp.where((earlier <= query) & (earlier > query - reach), 1.0, 0.0).astype(BF16)
    counts = jnp.minimum(query + 1, reach).astype(F32)
    scale = pool_s[...].astype(F32)
    for s in range(tokens // SEQ):
        rows = slice(s * SEQ, s * SEQ + SEQ)
        part = pooled[rows]
        window = jnp.dot(inside, part, preferred_element_type=F32)
        contrast = (window / counts - part.astype(F32)).astype(BF16)
        mixed = jnp.dot(contrast, pool_w[0], preferred_element_type=F32)
        group_out[rows, :] = (mixed * scale).astype(BF16)

    def mix_product(owner_x, owner_core, side):
        pair = mixer[owner_x, pl.ds(2 * owner_core, 2), 128:256, :]
        weights = jnp.concatenate([pair[0], pair[1]], axis=1)
        return jnp.dot(group_out[rows_of(side), :], weights, preferred_element_type=F32)

    r_mix.pair(mix_product)
    g_b.p2_own()
    r_mix.start(mix_product)
    r_mix.forward()
    g_a.p2_forward()

    def store_middle(side, value):
        blocks_b[mine, rows_of(side), :] = value

    r_mix.result(lambda side: blocks_a[mine, rows_of(side), :], store_middle)
    s_mid.start()
    g_b.p2_forward()
    g_down.p2_own()
    take(blocks_b, ffn_gain, mine, first=True)
    s_mid.from_core(6, 0)
    take(blocks_b, ffn_gain, s_mid.index(0, other=True))
    s_mid.forward()
    s_mid.near()
    for step in (3, 1):
        take(blocks_b, ffn_gain, s_mid.index(step))
    s_mid.far()
    take(blocks_b, ffn_gain, s_mid.index(2))
    for k, step in ((7, 3), (8, 1), (9, 2)):
        s_mid.from_core(k, step)
        take(blocks_b, ffn_gain, s_mid.index(step, other=True))
    row_rates()

    def units(buf, at, width, column):
        weights = buf[:, :, :, at : at + 2 * width].reshape(2048, 2 * width)

        def some(i, carry):
            rows = pl.ds(pl.multiple_of(i * 256, 256), 256)
            acts = jnp.dot(scaled[rows, :], weights, preferred_element_type=F32)
            rate = rates[rows, 0:width]
            gate, up = acts[:, :width] * rate, acts[:, width:] * rate
            hidden[rows, column : column + width] = (gate / (1.0 + jnp.exp(-gate)) * up).astype(BF16)
            return carry

        lax.fori_loop(0, tokens // 256, some, 0)

    g_a.finish()
    for chunk in range(3):
        units(pair_a, 256 * chunk, 128, 128 * chunk)
    g_down.p2_forward()
    g_b.finish()
    for chunk in range(2):
        units(pair_b, 256 * chunk, 128, 384 + 128 * chunk)
    units(pair_b, 512, 64, 640)
    g_down.finish()

    def ffn_product(owner_x, owner_core, side):
        pair = down[owner_x, pl.ds(2 * owner_core, 2)]
        weights = jnp.concatenate([pair[0], pair[1]], axis=1)
        return jnp.dot(hidden[rows_of(side), :], weights, preferred_element_type=F32)

    r_ffn.pair(ffn_product)
    r_ffn.start(ffn_product)
    r_ffn.forward()

    def store_result(side, value):
        out[rows_of(side), :] = value

    r_ffn.result(lambda side: blocks_b[mine, rows_of(side), :], store_result)

    for net in [g.net for g in gathers] + [s_in.net, s_mid.net, r_mix.net, r_ffn.net]:
        net.drain()


def on_device(stream, in_weight, pool_weight, pool_scale, out_weight, mix_gain, ffn_gain, gate_weight, up_weight, down_weight):
    tokens = stream.shape[0]
    half = tokens // 2
    return pl.pallas_call(
        kernel,
        out_shape=jax.ShapeDtypeStruct(stream.shape, BF16),
        in_specs=[pl.BlockSpec(memory_space=pltpu.HBM)] * 10,
        out_specs=pl.BlockSpec(memory_space=pltpu.VMEM),
        scratch_shapes=[
            pltpu.VMEM((2, 16, 128), BF16),
            pltpu.VMEM((16, 128), F32),
            pltpu.VMEM((16, 128), F32),
            pltpu.VMEM((704, 128), BF16),
            pltpu.VMEM((704, 128), BF16),
            pltpu.VMEM((1, 128, 128), BF16),
            pltpu.VMEM((1, 128), BF16),
            pltpu.VMEM((4, 4, 256, 128), BF16),
            pltpu.VMEM((4, 4, 128, 768), BF16),
            pltpu.VMEM((4, 4, 128, 640), BF16),
            pltpu.VMEM((4, 4, 704, 128), BF16),
            pltpu.VMEM((8, tokens, 256), BF16),
            pltpu.VMEM((8, tokens, 256), BF16),
            pltpu.VMEM((tokens, 2048), BF16),
            pltpu.VMEM((tokens, 128), F32),
            pltpu.VMEM((tokens, 128), F32),
            pltpu.VMEM((tokens, 128), BF16),
            pltpu.VMEM((tokens, 704), BF16),
            pltpu.VMEM((2, 4, tokens, 256), BF16),
            pltpu.VMEM((2, 4, tokens, 256), BF16),
            pltpu.VMEM((2, 3, tokens, 256), BF16),
            pltpu.VMEM((tokens, 256), F32),
            pltpu.VMEM((2, 2, half, 256), BF16),
            pltpu.VMEM((2, 6, half, 256), BF16),
            pltpu.SemaphoreType.DMA((10,)),
            pltpu.SemaphoreType.DMA((4, 20)),
            pltpu.SemaphoreType.DMA((4, 20)),
            pltpu.SemaphoreType.DMA((2, 20)),
            pltpu.SemaphoreType.DMA((2, 20)),
        ],
        compiler_params=pltpu.CompilerParams(
            collective_id=0, has_side_effects=True, vmem_limit_bytes=40 * 1024 * 1024
        ),
    )(*(pltpu.with_memory_space_constraint(a, pltpu.HBM) for a in (
        stream, in_weight, pool_weight, pool_scale.reshape(1, -1), out_weight,
        mix_gain.reshape(16, 128), ffn_gain.reshape(16, 128), gate_weight.T, up_weight.T, down_weight,
    )))


def solution(mesh):
    finer = Mesh(
        mesh.devices.reshape(mesh.shape["rep"], RING, RING, RING, 2),
        ("rep", "fs_0", "fs_1", "x", "core"),
    )
    fs, tp = ("fs_0", "fs_1"), ("x", "core")
    rows = ("rep", *fs)
    return jax.shard_map(
        on_device,
        mesh=finer,
        in_specs=(
            P(rows, tp), P(fs, tp), P(tp, None, None), P(tp), P(tp, fs),
            P(), P(), P(fs, tp), P(fs, tp), P(tp, fs),
        ),
        out_specs=P(rows, tp),
        check_vma=False,
    )
```

```python
import jax
import jax.numpy as jnp
from jax import lax
from jax.experimental import pallas as pl
from jax.experimental.pallas import tpu as pltpu
from jax.sharding import Mesh
from jax.sharding import PartitionSpec as P

SEQ = 128
RING = 4
EPS = 1e-06
F32, BF16 = jnp.float32, jnp.bfloat16


class Place:
    def __init__(self):
        self.rep, self.z, self.y = (lax.axis_index(a) for a in ("rep", "fs_0", "fs_1"))
        self.x, self.core = lax.axis_index("x"), lax.axis_index("core")

    def to(self, axis, step):
        if axis == "core":
            return {"core": 1 - self.core}
        if axis == "z":
            deep = (self.rep * RING + self.z + step + 2 * RING) % (2 * RING)
            return {"rep": deep // RING, "fs_0": deep % RING}
        index = {"x": self.x, "y": self.y}[axis]
        return {{"x": "x", "y": "fs_1"}[axis]: (index + step + RING) % RING}


class Net:
    def __init__(self, place, fresh):
        self.place, self.fresh = place, fresh

    def send(self, src, dst, sent, landed, axis, step):
        pltpu.make_async_remote_copy(
            src_ref=src,
            dst_ref=dst,
            send_sem=sent,
            recv_sem=landed,
            device_id=self.place.to(axis, step),
            device_id_type=pl.DeviceIdType.MESH,
        ).start()

    def wait(self, semaphore, as_many):
        pltpu.make_async_copy(as_many, as_many, semaphore).wait()


class Gather(Net):
    def __init__(self, place, fresh, buf):
        super().__init__(place, fresh)
        self.buf = buf
        half = buf.shape[2] // 2
        self.flows = (("y", "z", 0, half), ("z", "y", half, half))
        self.sent_1, self.sent_2, self.got_own, self.got_line, self.got_plane, self.got_all = (
            fresh() for _ in range(6)
        )

    def block(self, axis, step, first, rows):
        z, y = self.place.z, self.place.y
        z, y = ((z + step) % RING, y) if axis == "z" else (z, (y + step) % RING)
        return self.buf.at[z, y, pl.ds(first, rows), :]

    def plane(self, axis, step, side, first, rows):
        two = pl.ds(2 * side, 2)
        if axis == "z":
            return self.buf.at[(self.place.z + step) % RING, two, pl.ds(first, rows), :]
        return self.buf.at[two, (self.place.y + step) % RING, pl.ds(first, rows), :]

    def relay(self, part, sent, landed, axis, step):
        self.send(part, part, sent, landed, axis, step)

    def p1_own(self):
        for axis, _, first, rows in self.flows:
            own = self.block(axis, 0, first, rows)
            self.relay(own, self.sent_1, self.got_own, axis, 1)
            self.relay(own, self.sent_1, self.got_own, axis, -1)

    def p1_forward(self):
        self.wait(self.got_own, self.buf.at[0, pl.ds(0, 2)])
        for axis, _, first, rows in self.flows:
            half = (rows // 2 + 15) // 16 * 16
            self.relay(self.block(axis, 3, first, half), self.sent_1, self.got_line, axis, 1)
            self.relay(self.block(axis, 1, first + half, rows - half), self.sent_1, self.got_line, axis, -1)

    def p2_own(self):
        self.p2_first()
        self.p2_second()

    def p2_first(self):
        self.wait(self.got_line, self.buf.at[0, 0])
        for _, axis, first, rows in self.flows:
            low, high = (self.plane(axis, 0, side, first, rows) for side in (0, 1))
            self.relay(low, self.sent_2, self.got_plane, axis, 1)
            self.relay(high, self.sent_2, self.got_plane, axis, -1)

    def p2_second(self):
        for _, axis, first, rows in self.flows:
            low, high = (self.plane(axis, 0, side, first, rows) for side in (0, 1))
            self.relay(high, self.sent_2, self.got_all, axis, 1)
            self.relay(low, self.sent_2, self.got_all, axis, -1)

    def p2_forward(self):
        self.wait(self.got_plane, self.buf.at[0])
        for _, axis, first, rows in self.flows:
            self.relay(self.plane(axis, 3, 0, first, rows), self.sent_2, self.got_all, axis, 1)
            self.relay(self.plane(axis, 1, 1, first, rows), self.sent_2, self.got_all, axis, -1)

    def finish(self):
        self.wait(self.got_all, self.buf.at[pl.ds(0, 2)])

    def drain(self):
        self.wait(self.sent_1, self.buf.at[0, pl.ds(0, 3)])
        self.wait(self.sent_2, self.buf.at[pl.ds(0, 3)])


class Spread(Net):
    def __init__(self, place, fresh, buf, first, rows):
        super().__init__(place, fresh)
        self.buf, self.first, self.rows = buf, first, rows
        self.sent, self.got_0, self.got_1, self.got_2, self.pair_0, self.pair_1, self.pair_2 = (
            fresh() for _ in range(7)
        )

    def index(self, step, other=False):
        core = 1 - self.place.core if other else self.place.core
        return 2 * ((self.place.x + step) % RING) + core

    def relay(self, step, side, landed, to):
        half = self.rows // 2
        part = self.buf.at[self.index(step), pl.ds(self.first + side * half, half), :]
        self.send(part, part, self.sent, landed, "x", to)

    def to_core(self, step, landed):
        block = self.buf.at[self.index(step), pl.ds(self.first, self.rows), :]
        self.send(block, block, self.sent, landed, "core", 0)

    def blocks(self, count):
        return self.buf.at[pl.ds(0, count), pl.ds(self.first, self.rows), :]

    def start(self):
        self.relay(0, 0, self.got_0, 1)
        self.relay(0, 1, self.got_0, -1)
        self.relay(0, 1, self.got_1, 1)
        self.relay(0, 0, self.got_1, -1)
        self.to_core(0, self.pair_0)

    def forward(self):
        self.wait(self.got_0, self.blocks(1))
        self.relay(3, 0, self.got_2, 1)
        self.relay(1, 1, self.got_2, -1)

    def near(self):
        self.wait(self.got_1, self.blocks(1))
        self.to_core(3, self.pair_1)
        self.to_core(1, self.pair_1)

    def far(self):
        self.wait(self.got_2, self.blocks(1))
        self.to_core(2, self.pair_2)

    def other_own(self):
        self.wait(self.pair_0, self.blocks(1))

    def other_near(self):
        self.wait(self.pair_1, self.blocks(2))

    def other_far(self):
        self.wait(self.pair_2, self.blocks(1))

    def drain(self):
        self.wait(self.sent, self.blocks(7))


def kernel(
    stream, w_in, pool_w_in, pool_s_in, w_out, mix_gain_in, ffn_gain_in, w_gate, w_up, w_down, out,
    gains, mix_gain, ffn_gain, gate_in, up_in, down_in, pool_w, pool_s,
    mixer, pair_a, pair_b, down_a, down_b, blocks_a, blocks_b, scaled, squares, rates, group_out, hidden,
    out_0, in_0, sums_0, own_0, combined_0, landed_0,
    out_1, in_1, sums_1, own_1, combined_1, landed_1, total_1,
    out_2, in_2, sums_2, own_2, combined_2, landed_2,
    fetched, sems,
):
    place = Place()
    x, core, y, z = place.x, place.core, place.y, place.z
    mine = 2 * x + core
    tokens = stream.shape[0]

    barrier = pltpu.get_barrier_semaphore()
    neighbours = [place.to(a, s) for a in "xyz" for s in (1, -1)] + [place.to("core", 0)]
    for device in neighbours:
        pl.semaphore_signal(barrier, inc=1, device_id=device, device_id_type=pl.DeviceIdType.MESH)
    fetches = [
        pltpu.make_async_copy(src, dst, fetched.at[i])
        for i, (src, dst) in enumerate((
            (stream, blocks_a.at[mine]),
            (w_in, mixer.at[z, y, pl.ds(0, 128), :]),
            (w_out, mixer.at[z, y, pl.ds(128, 128), :]),
            (w_gate, gate_in),
            (w_up, up_in),
            (w_down, down_in),
            (mix_gain_in, gains.at[0]),
            (ffn_gain_in, gains.at[1]),
            (pool_w_in, pool_w),
            (pool_s_in, pool_s),
        ))
    ]
    for fetch in fetches:
        fetch.start()
    pl.semaphore_wait(barrier, len(neighbours))

    taken = iter(range(sems.shape[0]))

    def fresh():
        return sems.at[next(taken)]

    gathers = [Gather(place, fresh, buf) for buf in (mixer, pair_a, pair_b, down_a, down_b)]
    g_mix, g_a, g_b, g_da, g_db = gathers
    streams = (0, 1)
    rows_each = tokens // 2
    half = rows_each // 2
    s_in = [Spread(place, fresh, blocks_a, rows_each * t, rows_each) for t in streams]
    s_mid = [Spread(place, fresh, blocks_b, rows_each * t, rows_each) for t in streams]

    def take(spread, gain_ref, step, other=False, first=False):
        index = spread.index(step, other)
        lanes = pl.ds(pl.multiple_of(index * 256, 256), 256)
        gain = jnp.concatenate([gain_ref[pl.ds(2 * index + i, 1), :] for i in (0, 1)], axis=1)

        def some(i, carry):
            rows = pl.ds(pl.multiple_of(spread.first + i * 64, 64), 64)
            value = spread.buf[index, rows, :].astype(F32)
            scaled[rows, lanes] = (value * gain).astype(BF16)
            square = value * value
            square = square[:, :128] + square[:, 128:]
            squares[rows, :] = square if first else squares[rows, :] + square
            return carry

        lax.fori_loop(0, spread.rows // 64, some, 0)

    def row_rates(t):
        rows = slice(rows_each * t, rows_each * t + rows_each)
        total = jnp.sum(squares[rows, :], axis=1, keepdims=True)
        rates[rows, :] = jnp.broadcast_to(lax.rsqrt(total * (1.0 / 2048.0) + EPS), (rows_each, 128))

    def rows_of(side):
        return pl.ds(side * half, half)

    class Summed(Net):
        steps = (2, 1, 3, 0)

        def __init__(self, t, *buffers):
            super().__init__(place, fresh)
            self.out, self.into, self.sums, self.own, self.combined, self.landed = (
                buffer.at[t] for buffer in buffers
            )
            self.sent_pair, self.sent, self.pair_0, self.pair_1, self.got_far, self.got = (
                fresh() for _ in range(6)
            )

        def give(self):
            for j in range(4):
                landed = self.pair_1 if j else self.pair_0
                self.send(self.out.at[j], self.into.at[j], self.sent_pair, landed, "core", 0)

        def start(self):
            sums, landed = self.sums, self.landed
            for j in range(4):
                if j < 2:
                    self.wait(*((self.pair_0, self.into.at[0]), (self.pair_1, self.into.at[pl.ds(1, 3)]))[j])
                total = self.own[j] + self.into[j].astype(F32)
                if j == 3:
                    self.own[j] = total
                else:
                    sums[j] = total.astype(BF16)
                if j == 0:
                    self.send(sums.at[0, rows_of(0)], landed.at[0], self.sent, self.got_far, "x", 1)
                    self.send(sums.at[0, rows_of(1)], landed.at[1], self.sent, self.got_far, "x", -1)
                if j == 1:
                    self.send(sums.at[1, rows_of(1)], landed.at[2], self.sent, self.got, "x", 1)
                if j == 2:
                    self.send(sums.at[2, rows_of(0)], landed.at[3], self.sent, self.got, "x", -1)

        def forward(self):
            self.wait(self.got_far, self.landed.at[pl.ds(0, 2)])
            for side, step in ((0, 1), (1, -1)):
                total = self.sums[1 + side, rows_of(side), :].astype(F32) + self.landed[side].astype(F32)
                self.combined[side] = total.astype(BF16)
                self.send(self.combined.at[side], self.landed.at[4 + side], self.sent, self.got, "x", step)

        def result(self, store):
            self.wait(self.got, self.landed.at[pl.ds(2, 4)])
            for side in (0, 1):
                store(
                    side,
                    self.own[3, rows_of(side), :]
                    + self.landed[3 - side].astype(F32)
                    + self.landed[4 + side].astype(F32),
                )

        def drain(self):
            self.wait(self.sent_pair, self.out)
            self.wait(self.sent, self.sums)

    def pair_up(sums, products):
        for group in products.groups:
            for i, j, value in products(group, 1 - core):
                sums[i].out[j] = value.astype(BF16)
        for each in sums:
            each.give()
        for group in products.groups:
            for i, j, value in products(group, core):
                sums[i].own[j] = value

    r_mix = [Summed(t, out_0, in_0, sums_0, own_0, combined_0, landed_0) for t in streams]
    r_one = [Summed(t, out_1, in_1, sums_1, own_1, combined_1, landed_1) for t in streams]
    r_two = [Summed(t, out_2, in_2, sums_2, own_2, combined_2, landed_2) for t in streams]

    def token_rows(t, side):
        return pl.ds(rows_each * t + half * side, half)

    reach = jnp.where(x == 0, 2, jnp.where(x == 1, 4, jnp.where(x == 2, 8, 16)))

    def mix(t):
        first = rows_each * t
        pooled = jnp.dot(
            scaled[first : first + rows_each, :], mixer[:, :, 0:128, :].reshape(2048, 128),
            preferred_element_type=F32,
        )
        pooled = (pooled * rates[first : first + rows_each, :]).astype(BF16)
        query = lax.broadcasted_iota(jnp.int32, (SEQ, SEQ), 0)
        earlier = lax.broadcasted_iota(jnp.int32, (SEQ, SEQ), 1)
        inside = jnp.where((earlier <= query) & (earlier > query - reach), 1.0, 0.0).astype(BF16)
        counts = jnp.minimum(query + 1, reach).astype(F32)
        scale = pool_s[...].astype(F32)
        for s in range(rows_each // SEQ):
            part = pooled[s * SEQ : s * SEQ + SEQ]
            window = jnp.dot(inside, part, preferred_element_type=F32)
            contrast = (window / counts - part.astype(F32)).astype(BF16)
            mixed = jnp.dot(contrast, pool_w[0], preferred_element_type=F32)
            group_out[first + s * SEQ : first + s * SEQ + SEQ, :] = (mixed * scale).astype(BF16)

    def mix_products(t):
        first = rows_each * t

        def products(group, owner_core):
            for j in group:
                pair = mixer[(x + Summed.steps[j]) % RING, pl.ds(2 * owner_core, 2), 128:256, :]
                weights = jnp.concatenate([pair[0], pair[1]], axis=1)
                tokens_of = group_out[first : first + rows_each, :]
                yield 0, j, jnp.dot(tokens_of, weights, preferred_element_type=F32)

        products.groups = ((0,), (1,), (2,), (3,))
        return products

    def ffn_products(buf):
        def products(group, owner_core):
            columns = []
            for j in group:
                pair = buf[(x + Summed.steps[j]) % RING, pl.ds(2 * owner_core, 2)]
                early = jnp.concatenate([pair[0][:, :64], pair[1][:, :64]], axis=1)
                late = jnp.concatenate([pair[0][:, 64:], pair[1][:, 64:]], axis=1)
                columns.append(jnp.concatenate([early, late], axis=0))
            weights = jnp.concatenate(columns, axis=1)
            both = jnp.dot(hidden[...], weights, preferred_element_type=F32)
            for t in streams:
                for i, j in enumerate(group):
                    yield t, j, both[rows_each * t : rows_each * t + rows_each, 128 * i : 128 * i + 128]

        products.groups = ((0, 1), (2, 3))
        return products

    def units(t, buf, at, width, column):
        weights = buf[:, :, :, at : at + 2 * width].reshape(2048, 2 * width)
        rows = slice(rows_each * t, rows_each * t + rows_each)
        acts = jnp.dot(scaled[rows, :], weights, preferred_element_type=F32)
        rate = rates[rows, 0:width]
        gate, up = acts[:, :width] * rate, acts[:, width:] * rate
        hidden[rows, column : column + width] = (gate / (1.0 + jnp.exp(-gate)) * up).astype(BF16)

    def units_a(t):
        for chunk in range(3):
            units(t, pair_a, 256 * chunk, 128, 128 * chunk)

    def units_b(t):
        for chunk in range(2):
            units(t, pair_b, 256 * chunk, 128, 384 + 128 * chunk)
        units(t, pair_b, 512, 64, 640)

    def middle_of(t):
        def store(side, total):
            rows = token_rows(t, side)
            blocks_b[mine, rows, :] = (blocks_a[mine, rows, :].astype(F32) + total).astype(BF16)

        return store

    def first_of(t):
        def store(side, total):
            total_1[token_rows(t, side), :] = total

        return store

    def result_of(t):
        def store(side, second):
            rows = token_rows(t, side)
            first = total_1[rows, :]
            for i in (0, 1):
                lanes = slice(128 * i, 128 * i + 128)
                some = slice(64 * i, 64 * i + 64)
                total = jnp.concatenate([first[:, some], second[:, some]], axis=1)
                out[rows, lanes] = (blocks_b[mine, rows, lanes].astype(F32) + total).astype(BF16)

        return store

    fetches[0].wait()
    s_in[0].start()
    fetches[1].wait()
    fetches[2].wait()
    g_mix.p1_own()
    s_in[1].start()
    fetches[3].wait()
    fetches[4].wait()
    for tile in range(5):
        buf, at = (pair_a, tile) if tile < 3 else (pair_b, tile - 3)
        some = slice(128 * tile, 128 * tile + 128)
        buf[z, y, :, 256 * at : 256 * at + 128] = gate_in[some, :].T
        buf[z, y, :, 256 * at + 128 : 256 * at + 256] = up_in[some, :].T
    pair_b[z, y, :, 512:640] = jnp.concatenate([gate_in[640:704, :], up_in[640:704, :]], axis=0).T
    for fetch in fetches[5:]:
        fetch.wait()
    for lane, buf in ((0, down_a), (64, down_b)):
        some = slice(lane, lane + 64)
        buf[z, y] = jnp.concatenate([down_in[0:352, some], down_in[352:704, some]], axis=1)
    mix_gain[...] = gains[0].astype(F32)
    ffn_gain[...] = gains[1].astype(F32)
    g_a.p1_own()
    g_b.p1_own()
    for t in streams:
        take(s_in[t], mix_gain, 0, first=True)
    g_mix.p1_forward()
    g_da.p1_own()
    g_db.p1_own()
    s_in[0].forward()
    g_a.p1_forward()
    for t in streams:
        s_in[t].other_own()
        take(s_in[t], mix_gain, 0, other=True)
    g_mix.p2_own()
    g_b.p1_forward()
    s_in[0].near()
    s_in[1].forward()
    for step in (3, 1):
        take(s_in[0], mix_gain, step)
    s_in[1].near()
    g_mix.p2_forward()
    g_da.p1_forward()
    g_db.p1_forward()
    s_in[0].far()
    take(s_in[0], mix_gain, 2)
    for step in (3, 1):
        take(s_in[1], mix_gain, step)
    s_in[1].far()
    take(s_in[1], mix_gain, 2)
    g_a.p2_own()
    for t in streams:
        s_in[t].other_near()
        take(s_in[t], mix_gain, 3, other=True)
        take(s_in[t], mix_gain, 1, other=True)
        s_in[t].other_far()
        take(s_in[t], mix_gain, 2, other=True)
        row_rates(t)
    g_b.p2_own()
    g_mix.finish()
    mix(0)
    pair_up([r_mix[0]], mix_products(0))
    mix(1)
    r_mix[0].start()
    pair_up([r_mix[1]], mix_products(1))
    r_mix[1].start()
    r_mix[0].forward()
    r_mix[1].forward()
    r_mix[0].result(middle_of(0))
    s_mid[0].start()
    take(s_mid[0], ffn_gain, 0, first=True)
    g_a.p2_forward()
    g_b.p2_forward()
    r_mix[1].result(middle_of(1))
    s_mid[1].start()
    take(s_mid[1], ffn_gain, 0, first=True)
    g_da.p2_own()
    g_db.p2_first()
    for t in streams:
        s_mid[t].other_own()
        take(s_mid[t], ffn_gain, 0, other=True)
    s_mid[0].forward()
    s_mid[0].near()
    s_mid[1].forward()
    for step in (3, 1):
        take(s_mid[0], ffn_gain, step)
    s_mid[1].near()
    s_mid[0].far()
    take(s_mid[0], ffn_gain, 2)
    for step in (3, 1):
        take(s_mid[1], ffn_gain, step)
    s_mid[1].far()
    take(s_mid[1], ffn_gain, 2)
    for t in streams:
        s_mid[t].other_near()
        take(s_mid[t], ffn_gain, 3, other=True)
        take(s_mid[t], ffn_gain, 1, other=True)
        s_mid[t].other_far()
        take(s_mid[t], ffn_gain, 2, other=True)
        row_rates(t)
    g_a.finish()
    units_a(0)
    g_da.p2_forward()
    g_db.p2_second()
    units_a(1)
    g_b.finish()
    units_b(0)
    units_b(1)
    g_db.p2_forward()
    g_da.finish()
    pair_up(r_one, ffn_products(down_a))
    for t in streams:
        r_one[t].start()
    g_db.finish()
    pair_up(r_two, ffn_products(down_b))
    for t in streams:
        r_one[t].forward()
    for t in streams:
        r_two[t].start()
    for t in streams:
        r_one[t].result(first_of(t))
    for t in streams:
        r_two[t].forward()
    for t in streams:
        r_two[t].result(result_of(t))

    for net in [*gathers, *s_in, *s_mid, *r_mix, *r_one, *r_two]:
        net.drain()


def summing(tokens, width):
    rows = tokens // 2
    return [
        pltpu.VMEM((2, 4, rows, width), BF16),
        pltpu.VMEM((2, 4, rows, width), BF16),
        pltpu.VMEM((2, 3, rows, width), BF16),
        pltpu.VMEM((2, 4, rows, width), F32),
        pltpu.VMEM((2, 2, rows // 2, width), BF16),
        pltpu.VMEM((2, 6, rows // 2, width), BF16),
    ]


def on_device(stream, in_weight, pool_weight, pool_scale, out_weight, mix_gain, ffn_gain, gate_weight, up_weight, down_weight):
    tokens = stream.shape[0]
    return pl.pallas_call(
        kernel,
        out_shape=jax.ShapeDtypeStruct(stream.shape, BF16),
        in_specs=[pl.BlockSpec(memory_space=pltpu.HBM)] * 10,
        out_specs=pl.BlockSpec(memory_space=pltpu.VMEM),
        scratch_shapes=[
            pltpu.VMEM((2, 16, 128), BF16),
            pltpu.VMEM((16, 128), F32),
            pltpu.VMEM((16, 128), F32),
            pltpu.VMEM((704, 128), BF16),
            pltpu.VMEM((704, 128), BF16),
            pltpu.VMEM((704, 128), BF16),
            pltpu.VMEM((1, 128, 128), BF16),
            pltpu.VMEM((1, 128), BF16),
            pltpu.VMEM((4, 4, 256, 128), BF16),
            pltpu.VMEM((4, 4, 128, 768), BF16),
            pltpu.VMEM((4, 4, 128, 640), BF16),
            pltpu.VMEM((4, 4, 352, 128), BF16),
            pltpu.VMEM((4, 4, 352, 128), BF16),
            pltpu.VMEM((8, tokens, 256), BF16),
            pltpu.VMEM((8, tokens, 256), BF16),
            pltpu.VMEM((tokens, 2048), BF16),
            pltpu.VMEM((tokens, 128), F32),
            pltpu.VMEM((tokens, 128), F32),
            pltpu.VMEM((tokens, 128), BF16),
            pltpu.VMEM((tokens, 704), BF16),
            *summing(tokens, 256),
            *summing(tokens, 128),
            pltpu.VMEM((tokens, 128), F32),
            *summing(tokens, 128),
            pltpu.SemaphoreType.DMA((10,)),
            pltpu.SemaphoreType.DMA((94,)),
        ],
        compiler_params=pltpu.CompilerParams(
            collective_id=0, has_side_effects=True, vmem_limit_bytes=40 * 1024 * 1024
        ),
    )(*(pltpu.with_memory_space_constraint(a, pltpu.HBM) for a in (
        stream, in_weight, pool_weight, pool_scale.reshape(1, -1), out_weight,
        mix_gain.reshape(16, 128), ffn_gain.reshape(16, 128), gate_weight.T, up_weight.T, down_weight,
    )))


def solution(mesh):
    finer = Mesh(
        mesh.devices.reshape(mesh.shape["rep"], RING, RING, RING, 2),
        ("rep", "fs_0", "fs_1", "x", "core"),
    )
    fs, tp = ("fs_0", "fs_1"), ("x", "core")
    rows = ("rep", *fs)
    return jax.shard_map(
        on_device,
        mesh=finer,
        in_specs=(
            P(rows, tp), P(fs, tp), P(tp, None, None), P(tp), P(tp, fs),
            P(), P(), P(fs, tp), P(fs, tp), P(tp, fs),
        ),
        out_specs=P(rows, tp),
        check_vma=False,
    )
```

```python
import jax
import jax.numpy as jnp
from jax import lax
from jax.experimental import pallas as pl
from jax.experimental.pallas import tpu as pltpu
from jax.sharding import Mesh
from jax.sharding import PartitionSpec as P

SEQ = 128
RING = 4
EPS = 1e-06
F32, BF16 = jnp.float32, jnp.bfloat16


class Place:
    def __init__(self):
        self.rep, self.z, self.y = (lax.axis_index(a) for a in ("rep", "fs_0", "fs_1"))
        self.x, self.core = lax.axis_index("x"), lax.axis_index("core")

    def to(self, axis, step):
        if axis == "core":
            return {"core": 1 - self.core}
        if axis == "z":
            deep = (self.rep * RING + self.z + step + 2 * RING) % (2 * RING)
            return {"rep": deep // RING, "fs_0": deep % RING}
        index = {"x": self.x, "y": self.y}[axis]
        return {{"x": "x", "y": "fs_1"}[axis]: (index + step + RING) % RING}


class Net:
    def __init__(self, place, fresh, sent):
        self.place, self.fresh, self.sent = place, fresh, sent

    def send(self, src, dst, landed, axis, step):
        pltpu.make_async_remote_copy(
            src_ref=src,
            dst_ref=dst,
            send_sem=self.sent,
            recv_sem=landed,
            device_id=self.place.to(axis, step),
            device_id_type=pl.DeviceIdType.MESH,
        ).start()

    def wait(self, semaphore, as_many):
        pltpu.make_async_copy(as_many, as_many, semaphore).wait()


class Gather(Net):
    def __init__(self, place, fresh, sent, buf):
        super().__init__(place, fresh, sent)
        self.buf = buf
        half = buf.shape[2] // 2
        self.flows = (("y", "z", 0, half), ("z", "y", half, half))
        self.got_own, self.got_line, self.got_plane, self.got_all = (
            fresh() for _ in range(4)
        )

    def block(self, axis, step, first, rows):
        z, y = self.place.z, self.place.y
        z, y = ((z + step) % RING, y) if axis == "z" else (z, (y + step) % RING)
        return self.buf.at[z, y, pl.ds(first, rows), :]

    def plane(self, axis, step, side, first, rows):
        two = pl.ds(2 * side, 2)
        if axis == "z":
            return self.buf.at[(self.place.z + step) % RING, two, pl.ds(first, rows), :]
        return self.buf.at[two, (self.place.y + step) % RING, pl.ds(first, rows), :]

    def relay(self, part, landed, axis, step):
        self.send(part, part, landed, axis, step)

    def p1_own(self):
        for axis, _, first, rows in self.flows:
            own = self.block(axis, 0, first, rows)
            self.relay(own, self.got_own, axis, 1)
            self.relay(own, self.got_own, axis, -1)

    def p1_forward(self):
        self.wait(self.got_own, self.buf.at[0, pl.ds(0, 2)])
        for axis, _, first, rows in self.flows:
            half = (rows // 2 + 15) // 16 * 16
            self.relay(self.block(axis, 3, first, half), self.got_line, axis, 1)
            self.relay(self.block(axis, 1, first + half, rows - half), self.got_line, axis, -1)

    def p2_own(self):
        self.p2_first()
        self.p2_second()

    def p2_first(self):
        self.wait(self.got_line, self.buf.at[0, 0])
        for _, axis, first, rows in self.flows:
            low, high = (self.plane(axis, 0, side, first, rows) for side in (0, 1))
            self.relay(low, self.got_plane, axis, 1)
            self.relay(high, self.got_plane, axis, -1)

    def p2_second(self):
        for _, axis, first, rows in self.flows:
            low, high = (self.plane(axis, 0, side, first, rows) for side in (0, 1))
            self.relay(high, self.got_all, axis, 1)
            self.relay(low, self.got_all, axis, -1)

    def p2_forward(self):
        self.wait(self.got_plane, self.buf.at[0])
        for _, axis, first, rows in self.flows:
            self.relay(self.plane(axis, 3, 0, first, rows), self.got_all, axis, 1)
            self.relay(self.plane(axis, 1, 1, first, rows), self.got_all, axis, -1)

    def finish(self):
        self.wait(self.got_all, self.buf.at[pl.ds(0, 2)])


class Spread(Net):
    def __init__(self, place, fresh, sent, buf, first, rows):
        super().__init__(place, fresh, sent)
        self.buf, self.first, self.rows = buf, first, rows
        self.got_0, self.got_1, self.got_2, self.pair_0, self.pair_1, self.pair_2 = (
            fresh() for _ in range(6)
        )

    def index(self, step, other=False):
        core = 1 - self.place.core if other else self.place.core
        return 2 * ((self.place.x + step) % RING) + core

    def relay(self, step, side, landed, to):
        half = self.rows // 2
        part = self.buf.at[self.index(step), pl.ds(self.first + side * half, half), :]
        self.send(part, part, landed, "x", to)

    def to_core(self, step, landed):
        block = self.buf.at[self.index(step), pl.ds(self.first, self.rows), :]
        self.send(block, block, landed, "core", 0)

    def blocks(self, count):
        return self.buf.at[pl.ds(0, count), pl.ds(self.first, self.rows), :]

    def start(self):
        self.relay(0, 0, self.got_0, 1)
        self.relay(0, 1, self.got_0, -1)
        self.relay(0, 1, self.got_1, 1)
        self.relay(0, 0, self.got_1, -1)
        self.to_core(0, self.pair_0)

    def forward(self):
        self.wait(self.got_0, self.blocks(1))
        self.relay(3, 0, self.got_2, 1)
        self.relay(1, 1, self.got_2, -1)

    def near(self):
        self.wait(self.got_1, self.blocks(1))
        self.to_core(3, self.pair_1)
        self.to_core(1, self.pair_1)

    def far(self):
        self.wait(self.got_2, self.blocks(1))
        self.to_core(2, self.pair_2)

    def other_own(self):
        self.wait(self.pair_0, self.blocks(1))

    def other_near(self):
        self.wait(self.pair_1, self.blocks(2))

    def other_far(self):
        self.wait(self.pair_2, self.blocks(1))


def kernel(
    stream, w_in, pool_w_in, pool_s_in, w_out, mix_gain_in, ffn_gain_in, w_gate, w_up, w_down, out,
    gains, mix_gain, ffn_gain, gate_in, up_in, down_in, pool_w, pool_s,
    mixer_in, mixer_out, pair_a, pair_b, down_a, down_b, blocks_a, blocks_b, scaled, squares, rates, group_out, hidden,
    out_0, in_0, sums_0, own_0, combined_0, landed_0,
    out_1, in_1, sums_1, own_1, combined_1, landed_1, total_1,
    out_2, in_2, sums_2, own_2, combined_2, landed_2,
    tally, fetched, sems,
):
    place = Place()
    x, core, y, z = place.x, place.core, place.y, place.z
    mine = 2 * x + core
    tokens = stream.shape[0]

    barrier = pltpu.get_barrier_semaphore()
    neighbours = [place.to(a, s) for a in "xyz" for s in (1, -1)] + [place.to("core", 0)]
    for device in neighbours:
        pl.semaphore_signal(barrier, inc=1, device_id=device, device_id_type=pl.DeviceIdType.MESH)
    fetches = [
        pltpu.make_async_copy(src, dst, fetched.at[i])
        for i, (src, dst) in enumerate((
            (stream, blocks_a.at[mine]),
            (w_in, mixer_in.at[z, y]),
            (w_out, mixer_out.at[z, y]),
            (w_gate, gate_in),
            (w_up, up_in),
            (w_down, down_in),
            (mix_gain_in, gains.at[0]),
            (ffn_gain_in, gains.at[1]),
            (pool_w_in, pool_w),
            (pool_s_in, pool_s),
        ))
    ]
    for fetch in fetches:
        fetch.start()
    pl.semaphore_wait(barrier, len(neighbours))

    taken = iter(range(sems.shape[0]))

    def fresh():
        return sems.at[next(taken)]

    sent = fresh()
    gathers = [Gather(place, fresh, sent, buf) for buf in (mixer_in, mixer_out, pair_a, pair_b, down_a, down_b)]
    g_in, g_out, g_a, g_b, g_da, g_db = gathers
    streams = (0, 1)
    rows_each = tokens // 2
    half = rows_each // 2
    s_in = [Spread(place, fresh, sent, blocks_a, rows_each * t, rows_each) for t in streams]
    s_mid = [Spread(place, fresh, sent, blocks_b, rows_each * t, rows_each) for t in streams]

    def take(spread, gain_ref, step, other=False, first=False):
        index = spread.index(step, other)
        lanes = pl.ds(pl.multiple_of(index * 256, 256), 256)
        gain = jnp.concatenate([gain_ref[pl.ds(2 * index + i, 1), :] for i in (0, 1)], axis=1)

        def some(i, carry):
            rows = pl.ds(pl.multiple_of(spread.first + i * 64, 64), 64)
            value = spread.buf[index, rows, :].astype(F32)
            scaled[rows, lanes] = (value * gain).astype(BF16)
            square = value * value
            square = square[:, :128] + square[:, 128:]
            squares[rows, :] = square if first else squares[rows, :] + square
            return carry

        lax.fori_loop(0, spread.rows // 64, some, 0)

    def row_rates(t):
        rows = slice(rows_each * t, rows_each * t + rows_each)
        total = jnp.sum(squares[rows, :], axis=1, keepdims=True)
        rates[rows, :] = jnp.broadcast_to(lax.rsqrt(total * (1.0 / 2048.0) + EPS), (rows_each, 128))

    def rows_of(side):
        return pl.ds(side * half, half)

    class Summed(Net):
        steps = (2, 1, 3, 0)

        def __init__(self, t, *buffers):
            super().__init__(place, fresh, sent)
            self.out, self.into, self.sums, self.own, self.combined, self.landed = (
                buffer.at[t] for buffer in buffers
            )
            self.pair_0, self.pair_1, self.got_far, self.got = (
                fresh() for _ in range(4)
            )

        def give(self, j):
            landed = self.pair_1 if j else self.pair_0
            self.send(self.out.at[j], self.into.at[j], landed, "core", 0)

        def add(self, j):
            if j == 0:
                self.wait(self.pair_0, self.into.at[0])
            if j == 1:
                self.wait(self.pair_1, self.into.at[pl.ds(1, 3)])
            total = self.own[j] + self.into[j].astype(F32)
            if j == 3:
                self.own[j] = total
            else:
                self.sums[j] = total.astype(BF16)

        def start(self):
            sums, landed = self.sums, self.landed
            self.add(0)
            self.send(sums.at[0, rows_of(0)], landed.at[0], self.got_far, "x", 1)
            self.send(sums.at[0, rows_of(1)], landed.at[1], self.got_far, "x", -1)

        def start_near(self):
            sums, landed = self.sums, self.landed
            self.add(1)
            self.send(sums.at[1, rows_of(1)], landed.at[2], self.got, "x", 1)
            self.add(2)
            self.send(sums.at[2, rows_of(0)], landed.at[3], self.got, "x", -1)
            self.add(3)

        def forward(self):
            self.wait(self.got_far, self.landed.at[pl.ds(0, 2)])
            for side, step in ((0, 1), (1, -1)):
                total = self.sums[1 + side, rows_of(side), :].astype(F32) + self.landed[side].astype(F32)
                self.combined[side] = total.astype(BF16)
                self.send(self.combined.at[side], self.landed.at[4 + side], self.got, "x", step)

        def result(self, store):
            self.wait(self.got, self.landed.at[pl.ds(2, 4)])
            for side in (0, 1):
                store(
                    side,
                    self.own[3, rows_of(side), :]
                    + self.landed[3 - side].astype(F32)
                    + self.landed[4 + side].astype(F32),
                )


    def pair_up(sums, products):
        first, rest = products.groups

        def for_other(group):
            for i, j, value in products(group, 1 - core):
                sums[i].out[j] = value.astype(BF16)

        def for_this(group):
            for i, j, value in products(group, core):
                sums[i].own[j] = value

        def give(group):
            for j in group:
                for each in sums:
                    each.give(j)

        for_other(first)
        give(first)
        for_other(rest)
        for_this(first)
        give(rest)
        for each in sums:
            each.start()
        for_this(rest)

    r_mix = [Summed(t, out_0, in_0, sums_0, own_0, combined_0, landed_0) for t in streams]
    r_one = [Summed(t, out_1, in_1, sums_1, own_1, combined_1, landed_1) for t in streams]
    r_two = [Summed(t, out_2, in_2, sums_2, own_2, combined_2, landed_2) for t in streams]

    def token_rows(t, side):
        return pl.ds(rows_each * t + half * side, half)

    reach = jnp.where(x == 0, 2, jnp.where(x == 1, 4, jnp.where(x == 2, 8, 16)))

    def mix():
        pooled = jnp.dot(scaled[...], mixer_in[...].reshape(2048, 128), preferred_element_type=F32)
        pooled = (pooled * rates[...]).astype(BF16)
        query = lax.broadcasted_iota(jnp.int32, (SEQ, SEQ), 0)
        earlier = lax.broadcasted_iota(jnp.int32, (SEQ, SEQ), 1)
        inside = jnp.where((earlier <= query) & (earlier > query - reach), 1.0, 0.0).astype(BF16)
        counts = jnp.minimum(query + 1, reach).astype(F32)
        scale = pool_s[...].astype(F32)
        sequences = [pooled[s * SEQ : s * SEQ + SEQ] for s in range(tokens // SEQ)]
        windows = [jnp.dot(inside, part, preferred_element_type=F32) for part in sequences]
        contrasts = [
            (window / counts - part.astype(F32)).astype(BF16) for window, part in zip(windows, sequences)
        ]
        mixed = jnp.dot(jnp.concatenate(contrasts, axis=0), pool_w[0], preferred_element_type=F32)
        group_out[...] = (mixed * scale).astype(BF16)

    def mix_products(group, owner_core):
        columns = []
        for j in group:
            pair = mixer_out[(x + Summed.steps[j]) % RING, pl.ds(2 * owner_core, 2)]
            columns.append(jnp.concatenate([pair[0], pair[1]], axis=1))
        for i, j in enumerate(group):
            both = jnp.dot(group_out[...], columns[i], preferred_element_type=F32)
            for t in streams:
                yield t, j, both[rows_each * t : rows_each * t + rows_each]

    mix_products.groups = ((0, 1), (2, 3))

    def ffn_products(buf):
        def products(group, owner_core):
            columns = []
            for j in group:
                pair = buf[(x + Summed.steps[j]) % RING, pl.ds(2 * owner_core, 2)]
                early = jnp.concatenate([pair[0][:, :64], pair[1][:, :64]], axis=1)
                late = jnp.concatenate([pair[0][:, 64:], pair[1][:, 64:]], axis=1)
                columns.append(jnp.concatenate([early, late], axis=0))
            weights = jnp.concatenate(columns, axis=1)
            both = jnp.dot(hidden[...], weights, preferred_element_type=F32)
            for t in streams:
                for i, j in enumerate(group):
                    yield t, j, both[rows_each * t : rows_each * t + rows_each, 128 * i : 128 * i + 128]

        products.groups = ((0, 1), (2, 3))
        return products

    def units(chunks):
        before = None
        for chunk in (*chunks, None):
            acts = None
            if chunk is not None:
                t, buf, at, width, column = chunk
                rows = slice(rows_each * t, rows_each * t + rows_each)
                weights = buf[:, :, :, at : at + 2 * width].reshape(2048, 2 * width)
                acts = jnp.dot(scaled[rows, :], weights, preferred_element_type=F32)
            if before is not None:
                done, (t, _, _, width, column) = before
                rows = slice(rows_each * t, rows_each * t + rows_each)
                rate = rates[rows, 0:width]
                gate, up = done[:, :width] * rate, done[:, width:] * rate
                hidden[rows, column : column + width] = (gate / (1.0 + jnp.exp(-gate)) * up).astype(BF16)
            before = acts, chunk

    def units_a(t):
        units([(t, pair_a, 256 * i, 128, 128 * i) for i in range(3)])

    def units_b(t):
        last = (t, pair_b, 512, 64, 640)
        units([*((t, pair_b, 256 * i, 128, 384 + 128 * i) for i in range(2)), last])

    def middle_of(t):
        def store(side, total):
            rows = token_rows(t, side)
            blocks_b[mine, rows, :] = (blocks_a[mine, rows, :].astype(F32) + total).astype(BF16)

        return store

    def first_of(t):
        def store(side, total):
            total_1[token_rows(t, side), :] = total

        return store

    def result_of(t):
        def store(side, second):
            rows = token_rows(t, side)
            first = total_1[rows, :]
            for i in (0, 1):
                lanes = slice(128 * i, 128 * i + 128)
                some = slice(64 * i, 64 * i + 64)
                total = jnp.concatenate([first[:, some], second[:, some]], axis=1)
                out[rows, lanes] = (blocks_b[mine, rows, lanes].astype(F32) + total).astype(BF16)

        return store

    def down_relay():
        g_da.p2_forward()
        g_db.p2_second()

    fetches[0].wait()
    s_in[0].start()
    fetches[1].wait()
    fetches[2].wait()
    g_in.p1_own()
    g_out.p1_own()
    s_in[1].start()
    fetches[3].wait()
    fetches[4].wait()
    for tile in range(5):
        buf, at = (pair_a, tile) if tile < 3 else (pair_b, tile - 3)
        some = slice(128 * tile, 128 * tile + 128)
        buf[z, y, :, 256 * at : 256 * at + 128] = gate_in[some, :].T
        buf[z, y, :, 256 * at + 128 : 256 * at + 256] = up_in[some, :].T
    pair_b[z, y, :, 512:640] = jnp.concatenate([gate_in[640:704, :], up_in[640:704, :]], axis=0).T
    for fetch in fetches[5:]:
        fetch.wait()
    for lane, buf in ((0, down_a), (64, down_b)):
        some = slice(lane, lane + 64)
        buf[z, y] = jnp.concatenate([down_in[0:352, some], down_in[352:704, some]], axis=1)
    mix_gain[...] = gains[0].astype(F32)
    ffn_gain[...] = gains[1].astype(F32)
    g_a.p1_own()
    g_b.p1_own()
    for t in streams:
        take(s_in[t], mix_gain, 0, first=True)
    g_in.p1_forward()
    g_out.p1_forward()
    g_da.p1_own()
    g_db.p1_own()
    s_in[0].forward()
    g_a.p1_forward()
    for t in streams:
        s_in[t].other_own()
        take(s_in[t], mix_gain, 0, other=True)
    s_in[0].near()
    s_in[1].forward()
    for step in (3, 1):
        take(s_in[0], mix_gain, step)
    g_in.p2_own()
    g_out.p2_own()
    g_b.p1_forward()
    s_in[1].near()
    for step in (3, 1):
        take(s_in[1], mix_gain, step)
    s_in[0].far()
    take(s_in[0], mix_gain, 2)
    s_in[1].far()
    take(s_in[1], mix_gain, 2)
    g_in.p2_forward()
    g_da.p1_forward()
    g_db.p1_forward()
    for t in streams:
        s_in[t].other_near()
        take(s_in[t], mix_gain, 3, other=True)
        take(s_in[t], mix_gain, 1, other=True)
        s_in[t].other_far()
        take(s_in[t], mix_gain, 2, other=True)
        row_rates(t)
    g_out.p2_forward()
    g_a.p2_own()
    g_in.finish()
    mix()
    g_out.finish()
    pair_up(r_mix, mix_products)
    r_mix[0].start_near()
    r_mix[1].start_near()
    g_b.p2_own()
    r_mix[0].forward()
    r_mix[1].forward()
    g_a.p2_forward()
    r_mix[0].result(middle_of(0))
    s_mid[0].start()
    take(s_mid[0], ffn_gain, 0, first=True)
    g_b.p2_forward()
    r_mix[1].result(middle_of(1))
    s_mid[1].start()
    take(s_mid[1], ffn_gain, 0, first=True)
    g_da.p2_own()
    g_db.p2_first()
    for t in streams:
        s_mid[t].other_own()
        take(s_mid[t], ffn_gain, 0, other=True)
    s_mid[0].forward()
    s_mid[0].near()
    s_mid[1].forward()
    for step in (3, 1):
        take(s_mid[0], ffn_gain, step)
    s_mid[1].near()
    s_mid[0].far()
    take(s_mid[0], ffn_gain, 2)
    for step in (3, 1):
        take(s_mid[1], ffn_gain, step)
    s_mid[1].far()
    take(s_mid[1], ffn_gain, 2)
    for t in streams:
        s_mid[t].other_near()
        take(s_mid[t], ffn_gain, 3, other=True)
        take(s_mid[t], ffn_gain, 1, other=True)
        s_mid[t].other_far()
        take(s_mid[t], ffn_gain, 2, other=True)
        row_rates(t)
    g_a.finish()
    units_a(0)
    down_relay()
    units_a(1)
    g_b.finish()
    units_b(0)
    units_b(1)
    g_db.p2_forward()
    g_da.finish()
    pair_up(r_one, ffn_products(down_a))
    for t in streams:
        r_one[t].start_near()
    g_db.finish()
    pair_up(r_two, ffn_products(down_b))
    for t in streams:
        r_one[t].forward()
    for t in streams:
        r_two[t].start_near()
    for t in streams:
        r_two[t].forward()
    for t in streams:
        r_one[t].result(first_of(t))
    for t in streams:
        r_two[t].result(result_of(t))

    pltpu.make_async_copy(tally, tally, sent).wait()


def summing(tokens, width):
    rows = tokens // 2
    return [
        pltpu.VMEM((2, 4, rows, width), BF16),
        pltpu.VMEM((2, 4, rows, width), BF16),
        pltpu.VMEM((2, 3, rows, width), BF16),
        pltpu.VMEM((2, 4, rows, width), F32),
        pltpu.VMEM((2, 2, rows // 2, width), BF16),
        pltpu.VMEM((2, 6, rows // 2, width), BF16),
    ]


def sent_rows(tokens):
    weights = 128 + 128 + 128 * 6 + 128 * 5 + 352 + 352
    return 15 * weights + 7 * tokens * 2 * (2 + 1) + 7 * tokens * 2


def on_device(stream, in_weight, pool_weight, pool_scale, out_weight, mix_gain, ffn_gain, gate_weight, up_weight, down_weight):
    tokens = stream.shape[0]
    return pl.pallas_call(
        kernel,
        out_shape=jax.ShapeDtypeStruct(stream.shape, BF16),
        in_specs=[pl.BlockSpec(memory_space=pltpu.HBM)] * 10,
        out_specs=pl.BlockSpec(memory_space=pltpu.VMEM),
        scratch_shapes=[
            pltpu.VMEM((2, 16, 128), BF16),
            pltpu.VMEM((16, 128), F32),
            pltpu.VMEM((16, 128), F32),
            pltpu.VMEM((704, 128), BF16),
            pltpu.VMEM((704, 128), BF16),
            pltpu.VMEM((704, 128), BF16),
            pltpu.VMEM((1, 128, 128), BF16),
            pltpu.VMEM((1, 128), BF16),
            pltpu.VMEM((4, 4, 128, 128), BF16),
            pltpu.VMEM((4, 4, 128, 128), BF16),
            pltpu.VMEM((4, 4, 128, 768), BF16),
            pltpu.VMEM((4, 4, 128, 640), BF16),
            pltpu.VMEM((4, 4, 352, 128), BF16),
            pltpu.VMEM((4, 4, 352, 128), BF16),
            pltpu.VMEM((8, tokens, 256), BF16),
            pltpu.VMEM((8, tokens, 256), BF16),
            pltpu.VMEM((tokens, 2048), BF16),
            pltpu.VMEM((tokens, 128), F32),
            pltpu.VMEM((tokens, 128), F32),
            pltpu.VMEM((tokens, 128), BF16),
            pltpu.VMEM((tokens, 704), BF16),
            *summing(tokens, 256),
            *summing(tokens, 128),
            pltpu.VMEM((tokens, 128), F32),
            *summing(tokens, 128),
            pltpu.VMEM((sent_rows(tokens), 128), BF16),
            pltpu.SemaphoreType.DMA((10,)),
            pltpu.SemaphoreType.DMA((73,)),
        ],
        compiler_params=pltpu.CompilerParams(
            collective_id=0, has_side_effects=True, vmem_limit_bytes=48 * 1024 * 1024
        ),
    )(*(pltpu.with_memory_space_constraint(a, pltpu.HBM) for a in (
        stream, in_weight, pool_weight, pool_scale.reshape(1, -1), out_weight,
        mix_gain.reshape(16, 128), ffn_gain.reshape(16, 128), gate_weight.T, up_weight.T, down_weight,
    )))


def solution(mesh):
    finer = Mesh(
        mesh.devices.reshape(mesh.shape["rep"], RING, RING, RING, 2),
        ("rep", "fs_0", "fs_1", "x", "core"),
    )
    fs, tp = ("fs_0", "fs_1"), ("x", "core")
    rows = ("rep", *fs)
    return jax.shard_map(
        on_device,
        mesh=finer,
        in_specs=(
            P(rows, tp), P(fs, tp), P(tp, None, None), P(tp), P(tp, fs),
            P(), P(), P(fs, tp), P(fs, tp), P(tp, fs),
        ),
        out_specs=P(rows, tp),
        check_vma=False,
    )
```

```python
import jax
import jax.numpy as jnp
from jax import lax
from jax.experimental import pallas as pl
from jax.experimental.pallas import tpu as pltpu
from jax.sharding import Mesh
from jax.sharding import PartitionSpec as P

SEQ = 128
RING = 4
EPS = 1e-06
F32, BF16 = jnp.float32, jnp.bfloat16


class Place:
    def __init__(self):
        self.rep, self.z, self.y = (lax.axis_index(a) for a in ("rep", "fs_0", "fs_1"))
        self.x, self.core = lax.axis_index("x"), lax.axis_index("core")

    def to(self, axis, step):
        if axis == "core":
            return {"core": 1 - self.core}
        if axis == "z":
            deep = (self.rep * RING + self.z + step + 2 * RING) % (2 * RING)
            return {"rep": deep // RING, "fs_0": deep % RING}
        index = {"x": self.x, "y": self.y}[axis]
        return {{"x": "x", "y": "fs_1"}[axis]: (index + step + RING) % RING}


class Net:
    def __init__(self, place, fresh, sent):
        self.place, self.fresh, self.sent = place, fresh, sent

    def send(self, src, dst, landed, axis, step):
        pltpu.make_async_remote_copy(
            src_ref=src,
            dst_ref=dst,
            send_sem=self.sent,
            recv_sem=landed,
            device_id=self.place.to(axis, step),
            device_id_type=pl.DeviceIdType.MESH,
        ).start()

    def wait(self, semaphore, as_many):
        pltpu.make_async_copy(as_many, as_many, semaphore).wait()


class Gather(Net):
    def __init__(self, place, fresh, sent, buf):
        super().__init__(place, fresh, sent)
        self.buf = buf
        half = buf.shape[2] // 2
        self.flows = (("y", "z", 0, half), ("z", "y", half, half))
        self.got_own, self.got_line, self.got_plane, self.got_all = (
            fresh() for _ in range(4)
        )

    def block(self, axis, step, first, rows):
        z, y = self.place.z, self.place.y
        z, y = ((z + step) % RING, y) if axis == "z" else (z, (y + step) % RING)
        return self.buf.at[z, y, pl.ds(first, rows), :]

    def plane(self, axis, step, side, first, rows):
        two = pl.ds(2 * side, 2)
        if axis == "z":
            return self.buf.at[(self.place.z + step) % RING, two, pl.ds(first, rows), :]
        return self.buf.at[two, (self.place.y + step) % RING, pl.ds(first, rows), :]

    def relay(self, part, landed, axis, step):
        self.send(part, part, landed, axis, step)

    def p1_own(self):
        for axis, _, first, rows in self.flows:
            own = self.block(axis, 0, first, rows)
            self.relay(own, self.got_own, axis, 1)
            self.relay(own, self.got_own, axis, -1)

    def p1_forward(self):
        self.wait(self.got_own, self.buf.at[0, pl.ds(0, 2)])
        for axis, _, first, rows in self.flows:
            half = (rows // 2 + 15) // 16 * 16
            self.relay(self.block(axis, 3, first, half), self.got_line, axis, 1)
            self.relay(self.block(axis, 1, first + half, rows - half), self.got_line, axis, -1)

    def p2_own(self):
        self.p2_first()
        self.p2_second()

    def p2_first(self):
        self.wait(self.got_line, self.buf.at[0, 0])
        for _, axis, first, rows in self.flows:
            low, high = (self.plane(axis, 0, side, first, rows) for side in (0, 1))
            self.relay(low, self.got_plane, axis, 1)
            self.relay(high, self.got_plane, axis, -1)

    def p2_second(self):
        for _, axis, first, rows in self.flows:
            low, high = (self.plane(axis, 0, side, first, rows) for side in (0, 1))
            self.relay(high, self.got_all, axis, 1)
            self.relay(low, self.got_all, axis, -1)

    def p2_forward(self):
        self.wait(self.got_plane, self.buf.at[0])
        for _, axis, first, rows in self.flows:
            self.relay(self.plane(axis, 3, 0, first, rows), self.got_all, axis, 1)
            self.relay(self.plane(axis, 1, 1, first, rows), self.got_all, axis, -1)

    def finish(self):
        self.wait(self.got_all, self.buf.at[pl.ds(0, 2)])


class Spread(Net):
    def __init__(self, place, fresh, sent, buf, first, rows):
        super().__init__(place, fresh, sent)
        self.buf, self.first, self.rows = buf, first, rows
        self.got_0, self.got_1, self.got_2, self.pair_0, self.pair_1, self.pair_2 = (
            fresh() for _ in range(6)
        )

    def index(self, step, other=False):
        core = 1 - self.place.core if other else self.place.core
        return 2 * ((self.place.x + step) % RING) + core

    def relay(self, step, side, landed, to):
        half = self.rows // 2
        part = self.buf.at[self.index(step), pl.ds(self.first + side * half, half), :]
        self.send(part, part, landed, "x", to)

    def to_core(self, step, landed):
        block = self.buf.at[self.index(step), pl.ds(self.first, self.rows), :]
        self.send(block, block, landed, "core", 0)

    def blocks(self, count):
        return self.buf.at[pl.ds(0, count), pl.ds(self.first, self.rows), :]

    def start(self):
        self.relay(0, 0, self.got_0, 1)
        self.relay(0, 1, self.got_0, -1)
        self.relay(0, 1, self.got_1, 1)
        self.relay(0, 0, self.got_1, -1)
        self.to_core(0, self.pair_0)

    def forward(self):
        self.wait(self.got_0, self.blocks(1))
        self.relay(3, 0, self.got_2, 1)
        self.relay(1, 1, self.got_2, -1)

    def near(self):
        self.wait(self.got_1, self.blocks(1))
        self.to_core(3, self.pair_1)
        self.to_core(1, self.pair_1)

    def far(self):
        self.wait(self.got_2, self.blocks(1))
        self.to_core(2, self.pair_2)

    def other_own(self):
        self.wait(self.pair_0, self.blocks(1))

    def other_near(self):
        self.wait(self.pair_1, self.blocks(2))

    def other_far(self):
        self.wait(self.pair_2, self.blocks(1))


def kernel(
    stream, w_in, pool_w_in, pool_s_in, w_out, mix_gain_in, ffn_gain_in, w_gate, w_up, w_down, out,
    gains, mix_gain, ffn_gain, gate_in, up_in, down_in, pool_w, pool_s,
    mixer_in, mixer_out, pair_a, pair_b, down_a, down_b, blocks_a, blocks_b, scaled, squares, rates, group_out, hidden,
    out_0, in_0, sums_0, own_0, combined_0, landed_0,
    out_1, in_1, sums_1, own_1, combined_1, landed_1, total_1,
    out_2, in_2, sums_2, own_2, combined_2, landed_2,
    tally, fetched, sems,
):
    place = Place()
    x, core, y, z = place.x, place.core, place.y, place.z
    mine = 2 * x + core
    tokens = stream.shape[0]

    barrier = pltpu.get_barrier_semaphore()
    neighbours = [place.to(a, s) for a in "xyz" for s in (1, -1)] + [place.to("core", 0)]
    for device in neighbours:
        pl.semaphore_signal(barrier, inc=1, device_id=device, device_id_type=pl.DeviceIdType.MESH)
    fetches = [
        pltpu.make_async_copy(src, dst, fetched.at[i])
        for i, (src, dst) in enumerate((
            (stream, blocks_a.at[mine]),
            (w_in, mixer_in.at[z, y]),
            (w_out, mixer_out.at[z, y]),
            (w_gate, gate_in),
            (w_up, up_in),
            (w_down, down_in),
            (mix_gain_in, gains.at[0]),
            (ffn_gain_in, gains.at[1]),
            (pool_w_in, pool_w),
            (pool_s_in, pool_s),
        ))
    ]
    for fetch in fetches:
        fetch.start()
    pl.semaphore_wait(barrier, len(neighbours))

    taken = iter(range(sems.shape[0]))

    def fresh():
        return sems.at[next(taken)]

    sent = fresh()
    gathers = [Gather(place, fresh, sent, buf) for buf in (mixer_in, mixer_out, pair_a, pair_b, down_a, down_b)]
    g_in, g_out, g_a, g_b, g_da, g_db = gathers
    streams = (0, 1)
    rows_each = tokens // 2
    half = rows_each // 2
    s_in = [Spread(place, fresh, sent, blocks_a, rows_each * t, rows_each) for t in streams]
    s_mid = [Spread(place, fresh, sent, blocks_b, rows_each * t, rows_each) for t in streams]

    def take(spread, gain_ref, step, other=False, first=False):
        index = spread.index(step, other)
        lanes = pl.ds(pl.multiple_of(index * 256, 256), 256)
        gain = jnp.concatenate([gain_ref[pl.ds(2 * index + i, 1), :] for i in (0, 1)], axis=1)

        def some(i, carry):
            rows = pl.ds(pl.multiple_of(spread.first + i * 64, 64), 64)
            value = spread.buf[index, rows, :].astype(F32)
            scaled[rows, lanes] = (value * gain).astype(BF16)
            square = value * value
            square = square[:, :128] + square[:, 128:]
            squares[rows, :] = square if first else squares[rows, :] + square
            return carry

        lax.fori_loop(0, spread.rows // 64, some, 0)

    def row_rates(t):
        rows = slice(rows_each * t, rows_each * t + rows_each)
        total = jnp.sum(squares[rows, :], axis=1, keepdims=True)
        rates[rows, :] = jnp.broadcast_to(lax.rsqrt(total * (1.0 / 2048.0) + EPS), (rows_each, 128))

    def rows_of(side):
        return pl.ds(side * half, half)

    class Summed(Net):
        steps = (2, 1, 3, 0)

        def __init__(self, t, *buffers):
            super().__init__(place, fresh, sent)
            self.out, self.into, self.sums, self.own, self.combined, self.landed = (
                buffer.at[t] for buffer in buffers
            )
            self.pair_0, self.pair_1, self.got_far, self.got = (
                fresh() for _ in range(4)
            )

        def give(self, j):
            landed = self.pair_1 if j else self.pair_0
            self.send(self.out.at[j], self.into.at[j], landed, "core", 0)

        def add(self, j):
            if j == 0:
                self.wait(self.pair_0, self.into.at[0])
            if j == 1:
                self.wait(self.pair_1, self.into.at[pl.ds(1, 3)])
            total = self.own[j] + self.into[j].astype(F32)
            if j == 3:
                self.own[j] = total
            else:
                self.sums[j] = total.astype(BF16)

        def start(self):
            sums, landed = self.sums, self.landed
            self.add(0)
            self.send(sums.at[0, rows_of(0)], landed.at[0], self.got_far, "x", 1)
            self.send(sums.at[0, rows_of(1)], landed.at[1], self.got_far, "x", -1)

        def start_near(self):
            sums, landed = self.sums, self.landed
            self.add(1)
            self.send(sums.at[1, rows_of(1)], landed.at[2], self.got, "x", 1)
            self.add(2)
            self.send(sums.at[2, rows_of(0)], landed.at[3], self.got, "x", -1)
            self.add(3)

        def forward(self):
            self.wait(self.got_far, self.landed.at[pl.ds(0, 2)])
            for side, step in ((0, 1), (1, -1)):
                total = self.sums[1 + side, rows_of(side), :].astype(F32) + self.landed[side].astype(F32)
                self.combined[side] = total.astype(BF16)
                self.send(self.combined.at[side], self.landed.at[4 + side], self.got, "x", step)

        def result(self, store):
            self.wait(self.got, self.landed.at[pl.ds(2, 4)])
            for side in (0, 1):
                store(
                    side,
                    self.own[3, rows_of(side), :]
                    + self.landed[3 - side].astype(F32)
                    + self.landed[4 + side].astype(F32),
                )


    def pair_up(sums, products):
        first, rest = products.groups

        def for_other(group):
            for i, j, value in products(group, 1 - core):
                sums[i].out[j] = value.astype(BF16)

        def for_this(group):
            for i, j, value in products(group, core):
                sums[i].own[j] = value

        def give(group):
            for j in group:
                for each in sums:
                    each.give(j)

        for_other(first)
        give(first)
        for_other(rest)
        for_this(first)
        give(rest)
        for each in sums:
            each.start()
        for_this(rest)

    r_mix = [Summed(t, out_0, in_0, sums_0, own_0, combined_0, landed_0) for t in streams]
    r_one = [Summed(t, out_1, in_1, sums_1, own_1, combined_1, landed_1) for t in streams]
    r_two = [Summed(t, out_2, in_2, sums_2, own_2, combined_2, landed_2) for t in streams]

    def token_rows(t, side):
        return pl.ds(rows_each * t + half * side, half)

    reach = jnp.where(x == 0, 2, jnp.where(x == 1, 4, jnp.where(x == 2, 8, 16)))

    def mix():
        pooled = jnp.dot(scaled[...], mixer_in[...].reshape(2048, 128), preferred_element_type=F32)
        pooled = (pooled * rates[...]).astype(BF16)
        query = lax.broadcasted_iota(jnp.int32, (SEQ, SEQ), 0)
        earlier = lax.broadcasted_iota(jnp.int32, (SEQ, SEQ), 1)
        inside = jnp.where((earlier <= query) & (earlier > query - reach), 1.0, 0.0).astype(BF16)
        counts = jnp.minimum(query + 1, reach).astype(F32)
        scale = pool_s[...].astype(F32)
        sequences = [pooled[s * SEQ : s * SEQ + SEQ] for s in range(tokens // SEQ)]
        windows = [jnp.dot(inside, part, preferred_element_type=F32) for part in sequences]
        contrasts = [
            (window / counts - part.astype(F32)).astype(BF16) for window, part in zip(windows, sequences)
        ]
        mixed = jnp.dot(jnp.concatenate(contrasts, axis=0), pool_w[0], preferred_element_type=F32)
        group_out[...] = (mixed * scale).astype(BF16)

    def mix_products(group, owner_core):
        columns = []
        for j in group:
            pair = mixer_out[(x + Summed.steps[j]) % RING, pl.ds(2 * owner_core, 2)]
            columns.append(jnp.concatenate([pair[0], pair[1]], axis=1))
        for i, j in enumerate(group):
            both = jnp.dot(group_out[...], columns[i], preferred_element_type=F32)
            for t in streams:
                yield t, j, both[rows_each * t : rows_each * t + rows_each]

    mix_products.groups = ((0,), (1, 2, 3))

    def ffn_products(buf):
        def products(group, owner_core):
            columns = []
            for j in group:
                pair = buf[(x + Summed.steps[j]) % RING, pl.ds(2 * owner_core, 2)]
                early = jnp.concatenate([pair[0][:, :64], pair[1][:, :64]], axis=1)
                late = jnp.concatenate([pair[0][:, 64:], pair[1][:, 64:]], axis=1)
                columns.append(jnp.concatenate([early, late], axis=0))
            weights = jnp.concatenate(columns, axis=1)
            both = jnp.dot(hidden[...], weights, preferred_element_type=F32)
            for t in streams:
                for i, j in enumerate(group):
                    yield t, j, both[rows_each * t : rows_each * t + rows_each, 128 * i : 128 * i + 128]

        products.groups = ((0,), (1, 2, 3))
        return products

    def units(chunks):
        before = None
        for chunk in (*chunks, None):
            acts = None
            if chunk is not None:
                t, buf, at, width, column = chunk
                rows = slice(rows_each * t, rows_each * t + rows_each)
                weights = buf[:, :, :, at : at + 2 * width].reshape(2048, 2 * width)
                acts = jnp.dot(scaled[rows, :], weights, preferred_element_type=F32)
            if before is not None:
                done, (t, _, _, width, column) = before
                rows = slice(rows_each * t, rows_each * t + rows_each)
                rate = rates[rows, 0:width]
                gate, up = done[:, :width] * rate, done[:, width:] * rate
                hidden[rows, column : column + width] = (gate / (1.0 + jnp.exp(-gate)) * up).astype(BF16)
            before = acts, chunk

    def units_a(t):
        units([(t, pair_a, 256 * i, 128, 128 * i) for i in range(3)])

    def units_b(t):
        last = (t, pair_b, 512, 64, 640)
        units([*((t, pair_b, 256 * i, 128, 384 + 128 * i) for i in range(2)), last])

    def middle_of(t):
        def store(side, total):
            rows = token_rows(t, side)
            blocks_b[mine, rows, :] = (blocks_a[mine, rows, :].astype(F32) + total).astype(BF16)

        return store

    def first_of(t):
        def store(side, total):
            total_1[token_rows(t, side), :] = total

        return store

    def result_of(t):
        def store(side, second):
            rows = token_rows(t, side)
            first = total_1[rows, :]
            for i in (0, 1):
                lanes = slice(128 * i, 128 * i + 128)
                some = slice(64 * i, 64 * i + 64)
                total = jnp.concatenate([first[:, some], second[:, some]], axis=1)
                out[rows, lanes] = (blocks_b[mine, rows, lanes].astype(F32) + total).astype(BF16)

        return store

    def down_relay():
        g_da.p2_forward()
        g_db.p2_second()

    fetches[0].wait()
    s_in[0].start()
    fetches[1].wait()
    fetches[2].wait()
    g_in.p1_own()
    g_out.p1_own()
    s_in[1].start()
    fetches[3].wait()
    fetches[4].wait()
    for tile in range(5):
        buf, at = (pair_a, tile) if tile < 3 else (pair_b, tile - 3)
        some = slice(128 * tile, 128 * tile + 128)
        buf[z, y, :, 256 * at : 256 * at + 128] = gate_in[some, :].T
        buf[z, y, :, 256 * at + 128 : 256 * at + 256] = up_in[some, :].T
    pair_b[z, y, :, 512:640] = jnp.concatenate([gate_in[640:704, :], up_in[640:704, :]], axis=0).T
    for fetch in fetches[5:]:
        fetch.wait()
    for lane, buf in ((0, down_a), (64, down_b)):
        some = slice(lane, lane + 64)
        buf[z, y] = jnp.concatenate([down_in[0:352, some], down_in[352:704, some]], axis=1)
    mix_gain[...] = gains[0].astype(F32)
    ffn_gain[...] = gains[1].astype(F32)
    g_a.p1_own()
    g_b.p1_own()
    for t in streams:
        take(s_in[t], mix_gain, 0, first=True)
    g_in.p1_forward()
    g_out.p1_forward()
    g_da.p1_own()
    g_db.p1_own()
    s_in[0].forward()
    g_a.p1_forward()
    for t in streams:
        s_in[t].other_own()
        take(s_in[t], mix_gain, 0, other=True)
    s_in[0].near()
    s_in[1].forward()
    for step in (3, 1):
        take(s_in[0], mix_gain, step)
    g_in.p2_own()
    g_out.p2_own()
    g_b.p1_forward()
    s_in[1].near()
    for step in (3, 1):
        take(s_in[1], mix_gain, step)
    s_in[0].far()
    take(s_in[0], mix_gain, 2)
    s_in[1].far()
    take(s_in[1], mix_gain, 2)
    g_in.p2_forward()
    g_da.p1_forward()
    g_db.p1_forward()
    for t in streams:
        s_in[t].other_near()
        take(s_in[t], mix_gain, 3, other=True)
        take(s_in[t], mix_gain, 1, other=True)
        s_in[t].other_far()
        take(s_in[t], mix_gain, 2, other=True)
        row_rates(t)
    g_out.p2_forward()
    g_a.p2_own()
    g_in.finish()
    mix()
    g_out.finish()
    pair_up(r_mix, mix_products)
    r_mix[0].start_near()
    r_mix[1].start_near()
    g_b.p2_own()
    r_mix[0].forward()
    r_mix[1].forward()
    g_a.p2_forward()
    r_mix[0].result(middle_of(0))
    s_mid[0].start()
    take(s_mid[0], ffn_gain, 0, first=True)
    g_b.p2_forward()
    r_mix[1].result(middle_of(1))
    s_mid[1].start()
    take(s_mid[1], ffn_gain, 0, first=True)
    g_da.p2_own()
    g_db.p2_first()
    for t in streams:
        s_mid[t].other_own()
        take(s_mid[t], ffn_gain, 0, other=True)
    s_mid[0].forward()
    s_mid[0].near()
    s_mid[1].forward()
    for step in (3, 1):
        take(s_mid[0], ffn_gain, step)
    s_mid[1].near()
    s_mid[0].far()
    take(s_mid[0], ffn_gain, 2)
    for step in (3, 1):
        take(s_mid[1], ffn_gain, step)
    s_mid[1].far()
    take(s_mid[1], ffn_gain, 2)
    for t in streams:
        s_mid[t].other_near()
        take(s_mid[t], ffn_gain, 3, other=True)
        take(s_mid[t], ffn_gain, 1, other=True)
        s_mid[t].other_far()
        take(s_mid[t], ffn_gain, 2, other=True)
        row_rates(t)
    g_a.finish()
    units_a(0)
    down_relay()
    units_a(1)
    g_b.finish()
    units_b(0)
    units_b(1)
    g_db.p2_forward()
    g_da.finish()
    pair_up(r_one, ffn_products(down_a))
    for t in streams:
        r_one[t].start_near()
    g_db.finish()
    pair_up(r_two, ffn_products(down_b))
    for t in streams:
        r_one[t].forward()
    for t in streams:
        r_two[t].start_near()
    for t in streams:
        r_two[t].forward()
    for t in streams:
        r_one[t].result(first_of(t))
    for t in streams:
        r_two[t].result(result_of(t))

    pltpu.make_async_copy(tally, tally, sent).wait()


def summing(tokens, width):
    rows = tokens // 2
    return [
        pltpu.VMEM((2, 4, rows, width), BF16),
        pltpu.VMEM((2, 4, rows, width), BF16),
        pltpu.VMEM((2, 3, rows, width), BF16),
        pltpu.VMEM((2, 4, rows, width), F32),
        pltpu.VMEM((2, 2, rows // 2, width), BF16),
        pltpu.VMEM((2, 6, rows // 2, width), BF16),
    ]


def sent_rows(tokens):
    weights = 128 + 128 + 128 * 6 + 128 * 5 + 352 + 352
    return 15 * weights + 7 * tokens * 2 * (2 + 1) + 7 * tokens * 2


def on_device(stream, in_weight, pool_weight, pool_scale, out_weight, mix_gain, ffn_gain, gate_weight, up_weight, down_weight):
    tokens = stream.shape[0]
    return pl.pallas_call(
        kernel,
        out_shape=jax.ShapeDtypeStruct(stream.shape, BF16),
        in_specs=[pl.BlockSpec(memory_space=pltpu.HBM)] * 10,
        out_specs=pl.BlockSpec(memory_space=pltpu.VMEM),
        scratch_shapes=[
            pltpu.VMEM((2, 16, 128), BF16),
            pltpu.VMEM((16, 128), F32),
            pltpu.VMEM((16, 128), F32),
            pltpu.VMEM((704, 128), BF16),
            pltpu.VMEM((704, 128), BF16),
            pltpu.VMEM((704, 128), BF16),
            pltpu.VMEM((1, 128, 128), BF16),
            pltpu.VMEM((1, 128), BF16),
            pltpu.VMEM((4, 4, 128, 128), BF16),
            pltpu.VMEM((4, 4, 128, 128), BF16),
            pltpu.VMEM((4, 4, 128, 768), BF16),
            pltpu.VMEM((4, 4, 128, 640), BF16),
            pltpu.VMEM((4, 4, 352, 128), BF16),
            pltpu.VMEM((4, 4, 352, 128), BF16),
            pltpu.VMEM((8, tokens, 256), BF16),
            pltpu.VMEM((8, tokens, 256), BF16),
            pltpu.VMEM((tokens, 2048), BF16),
            pltpu.VMEM((tokens, 128), F32),
            pltpu.VMEM((tokens, 128), F32),
            pltpu.VMEM((tokens, 128), BF16),
            pltpu.VMEM((tokens, 704), BF16),
            *summing(tokens, 256),
            *summing(tokens, 128),
            pltpu.VMEM((tokens, 128), F32),
            *summing(tokens, 128),
            pltpu.VMEM((sent_rows(tokens), 128), BF16),
            pltpu.SemaphoreType.DMA((10,)),
            pltpu.SemaphoreType.DMA((73,)),
        ],
        compiler_params=pltpu.CompilerParams(
            collective_id=0, has_side_effects=True, vmem_limit_bytes=48 * 1024 * 1024
        ),
    )(*(pltpu.with_memory_space_constraint(a, pltpu.HBM) for a in (
        stream, in_weight, pool_weight, pool_scale.reshape(1, -1), out_weight,
        mix_gain.reshape(16, 128), ffn_gain.reshape(16, 128), gate_weight.T, up_weight.T, down_weight,
    )))


def solution(mesh):
    finer = Mesh(
        mesh.devices.reshape(mesh.shape["rep"], RING, RING, RING, 2),
        ("rep", "fs_0", "fs_1", "x", "core"),
    )
    fs, tp = ("fs_0", "fs_1"), ("x", "core")
    rows = ("rep", *fs)
    return jax.shard_map(
        on_device,
        mesh=finer,
        in_specs=(
            P(rows, tp), P(fs, tp), P(tp, None, None), P(tp), P(tp, fs),
            P(), P(), P(fs, tp), P(fs, tp), P(tp, fs),
        ),
        out_specs=P(rows, tp),
        check_vma=False,
    )
```

```python
import jax
import jax.numpy as jnp
from jax import lax
from jax.experimental import pallas as pl
from jax.experimental.pallas import tpu as pltpu
from jax.sharding import Mesh
from jax.sharding import PartitionSpec as P

SEQ = 128
RING = 4
EPS = 1e-06
F32, BF16 = jnp.float32, jnp.bfloat16


class Place:
    def __init__(self):
        self.rep, self.z, self.y = (lax.axis_index(a) for a in ("rep", "fs_0", "fs_1"))
        self.x, self.core = lax.axis_index("x"), lax.axis_index("core")

    def to(self, axis, step):
        if axis == "core":
            return {"core": 1 - self.core}
        if axis == "z":
            deep = (self.rep * RING + self.z + step + 2 * RING) % (2 * RING)
            return {"rep": deep // RING, "fs_0": deep % RING}
        index = {"x": self.x, "y": self.y}[axis]
        return {{"x": "x", "y": "fs_1"}[axis]: (index + step + RING) % RING}


class Net:
    def __init__(self, place, fresh, sent):
        self.place, self.fresh, self.sent = place, fresh, sent

    def send(self, src, dst, landed, axis, step):
        pltpu.make_async_remote_copy(
            src_ref=src,
            dst_ref=dst,
            send_sem=self.sent,
            recv_sem=landed,
            device_id=self.place.to(axis, step),
            device_id_type=pl.DeviceIdType.MESH,
        ).start()

    def wait(self, semaphore, as_many):
        pltpu.make_async_copy(as_many, as_many, semaphore).wait()


class Gather(Net):
    def __init__(self, place, fresh, sent, buf):
        super().__init__(place, fresh, sent)
        self.buf = buf
        half = buf.shape[2] // 2
        self.flows = (("y", "z", 0, half), ("z", "y", half, half))
        self.got_own, self.got_line, self.got_plane, self.got_all = (
            fresh() for _ in range(4)
        )

    def block(self, axis, step, first, rows):
        z, y = self.place.z, self.place.y
        z, y = ((z + step) % RING, y) if axis == "z" else (z, (y + step) % RING)
        return self.buf.at[z, y, pl.ds(first, rows), :]

    def plane(self, axis, step, side, first, rows):
        two = pl.ds(2 * side, 2)
        if axis == "z":
            return self.buf.at[(self.place.z + step) % RING, two, pl.ds(first, rows), :]
        return self.buf.at[two, (self.place.y + step) % RING, pl.ds(first, rows), :]

    def relay(self, part, landed, axis, step):
        self.send(part, part, landed, axis, step)

    def p1_own(self):
        for axis, _, first, rows in self.flows:
            own = self.block(axis, 0, first, rows)
            self.relay(own, self.got_own, axis, 1)
            self.relay(own, self.got_own, axis, -1)

    def p1_forward(self):
        self.wait(self.got_own, self.buf.at[0, pl.ds(0, 2)])
        for axis, _, first, rows in self.flows:
            half = (rows // 2 + 15) // 16 * 16
            self.relay(self.block(axis, 3, first, half), self.got_line, axis, 1)
            self.relay(self.block(axis, 1, first + half, rows - half), self.got_line, axis, -1)

    def p2_own(self):
        self.p2_first()
        self.p2_second()

    def p2_first(self):
        self.wait(self.got_line, self.buf.at[0, 0])
        for _, axis, first, rows in self.flows:
            low, high = (self.plane(axis, 0, side, first, rows) for side in (0, 1))
            self.relay(low, self.got_plane, axis, 1)
            self.relay(high, self.got_plane, axis, -1)

    def p2_second(self):
        for _, axis, first, rows in self.flows:
            low, high = (self.plane(axis, 0, side, first, rows) for side in (0, 1))
            self.relay(high, self.got_all, axis, 1)
            self.relay(low, self.got_all, axis, -1)

    def p2_forward(self):
        self.wait(self.got_plane, self.buf.at[0])
        for _, axis, first, rows in self.flows:
            self.relay(self.plane(axis, 3, 0, first, rows), self.got_all, axis, 1)
            self.relay(self.plane(axis, 1, 1, first, rows), self.got_all, axis, -1)

    def finish(self):
        self.wait(self.got_all, self.buf.at[pl.ds(0, 2)])


class Spread(Net):
    def __init__(self, place, fresh, sent, buf, first, rows):
        super().__init__(place, fresh, sent)
        self.buf, self.first, self.rows = buf, first, rows
        self.semaphores = [fresh() for _ in range(6)]
        self.got_0, self.got_1, self.got_2, self.pair_0, self.pair_1, self.pair_2 = self.semaphores

    def index(self, step, other=False):
        core = 1 - self.place.core if other else self.place.core
        return 2 * ((self.place.x + step) % RING) + core

    def relay(self, step, side, landed, to):
        half = self.rows // 2
        part = self.buf.at[self.index(step), pl.ds(self.first + side * half, half), :]
        self.send(part, part, landed, "x", to)

    def to_core(self, step, landed):
        block = self.buf.at[self.index(step), pl.ds(self.first, self.rows), :]
        self.send(block, block, landed, "core", 0)

    def blocks(self, count):
        return self.buf.at[pl.ds(0, count), pl.ds(self.first, self.rows), :]

    def start(self):
        self.relay(0, 0, self.got_0, 1)
        self.relay(0, 1, self.got_0, -1)
        self.relay(0, 1, self.got_1, 1)
        self.relay(0, 0, self.got_1, -1)
        self.to_core(0, self.pair_0)

    def forward(self):
        self.wait(self.got_0, self.blocks(1))
        self.relay(3, 0, self.got_2, 1)
        self.relay(1, 1, self.got_2, -1)

    def near(self):
        self.wait(self.got_1, self.blocks(1))
        self.to_core(3, self.pair_1)
        self.to_core(1, self.pair_1)

    def far(self):
        self.wait(self.got_2, self.blocks(1))
        self.to_core(2, self.pair_2)

    def other_own(self):
        self.wait(self.pair_0, self.blocks(1))

    def other_near(self):
        self.wait(self.pair_1, self.blocks(2))

    def other_far(self):
        self.wait(self.pair_2, self.blocks(1))


def kernel(
    stream, w_in, pool_w_in, pool_s_in, w_out, mix_gain_in, ffn_gain_in, w_gate, w_up, w_down, out,
    gains, mix_gain, ffn_gain, gate_in, up_in, down_in, pool_w, pool_s,
    mixer_in, mixer_out, pair_a, pair_b, down_a, down_b, blocks_a, blocks_b, scaled, squares, rates, group_out, hidden,
    out_0, in_0, sums_0, own_0, combined_0, landed_0,
    out_1, in_1, sums_1, own_1, combined_1, landed_1, total_1,
    out_2, in_2, sums_2, own_2, combined_2, landed_2,
    tally, fetched, sems,
):
    place = Place()
    x, core, y, z = place.x, place.core, place.y, place.z
    mine = 2 * x + core
    tokens = stream.shape[0]

    barrier = pltpu.get_barrier_semaphore()
    neighbours = [place.to(a, s) for a in "xyz" for s in (1, -1)] + [place.to("core", 0)]
    for device in neighbours:
        pl.semaphore_signal(barrier, inc=1, device_id=device, device_id_type=pl.DeviceIdType.MESH)
    fetches = [
        pltpu.make_async_copy(src, dst, fetched.at[i])
        for i, (src, dst) in enumerate((
            (stream, blocks_a.at[mine]),
            (w_in, mixer_in.at[z, y]),
            (w_out, mixer_out.at[z, y]),
            (w_gate, gate_in),
            (w_up, up_in),
            (w_down, down_in),
            (mix_gain_in, gains.at[0]),
            (ffn_gain_in, gains.at[1]),
            (pool_w_in, pool_w),
            (pool_s_in, pool_s),
        ))
    ]
    for fetch in fetches:
        fetch.start()
    pl.semaphore_wait(barrier, len(neighbours))

    taken = iter(range(sems.shape[0]))

    def fresh():
        return sems.at[next(taken)]

    def again(nets):
        used = iter([semaphore for net in nets for semaphore in net.semaphores])
        return lambda: next(used)

    sent = fresh()
    gathers = [Gather(place, fresh, sent, buf) for buf in (mixer_in, mixer_out, pair_a, pair_b, down_a, down_b)]
    g_in, g_out, g_a, g_b, g_da, g_db = gathers
    streams = (0, 1)
    rows_each = tokens // 2
    half = rows_each // 2
    s_in = [Spread(place, fresh, sent, blocks_a, rows_each * t, rows_each) for t in streams]
    old = again(s_in)
    s_mid = [Spread(place, old, sent, blocks_b, rows_each * t, rows_each) for t in streams]

    def take(spread, gain_ref, step, other=False, first=False):
        index = spread.index(step, other)
        lanes = pl.ds(pl.multiple_of(index * 256, 256), 256)
        gain = jnp.concatenate([gain_ref[pl.ds(2 * index + i, 1), :] for i in (0, 1)], axis=1)

        def some(i, carry):
            rows = pl.ds(pl.multiple_of(spread.first + i * 64, 64), 64)
            value = spread.buf[index, rows, :].astype(F32)
            scaled[rows, lanes] = (value * gain).astype(BF16)
            square = value * value
            square = square[:, :128] + square[:, 128:]
            squares[rows, :] = square if first else squares[rows, :] + square
            return carry

        lax.fori_loop(0, spread.rows // 64, some, 0)

    def row_rates(t):
        rows = slice(rows_each * t, rows_each * t + rows_each)
        total = jnp.sum(squares[rows, :], axis=1, keepdims=True)
        rates[rows, :] = jnp.broadcast_to(lax.rsqrt(total * (1.0 / 2048.0) + EPS), (rows_each, 128))

    def rows_of(side):
        return pl.ds(side * half, half)

    class Summed(Net):
        steps = (2, 1, 3, 0)

        def __init__(self, fresh, t, *buffers):
            super().__init__(place, fresh, sent)
            self.out, self.into, self.sums, self.own, self.combined, self.landed = (
                buffer.at[t] for buffer in buffers
            )
            self.semaphores = [fresh() for _ in range(4)]
            self.pair_0, self.pair_1, self.got_far, self.got = self.semaphores

        def give(self, j):
            landed = self.pair_1 if j else self.pair_0
            self.send(self.out.at[j], self.into.at[j], landed, "core", 0)

        def add(self, j):
            if j == 0:
                self.wait(self.pair_0, self.into.at[0])
            if j == 1:
                self.wait(self.pair_1, self.into.at[pl.ds(1, 3)])
            total = self.own[j] + self.into[j].astype(F32)
            if j == 3:
                self.own[j] = total
            else:
                self.sums[j] = total.astype(BF16)

        def start(self):
            sums, landed = self.sums, self.landed
            self.add(0)
            self.send(sums.at[0, rows_of(0)], landed.at[0], self.got_far, "x", 1)
            self.send(sums.at[0, rows_of(1)], landed.at[1], self.got_far, "x", -1)

        def start_near(self):
            sums, landed = self.sums, self.landed
            self.add(1)
            self.send(sums.at[1, rows_of(1)], landed.at[2], self.got, "x", 1)
            self.add(2)
            self.send(sums.at[2, rows_of(0)], landed.at[3], self.got, "x", -1)
            self.add(3)

        def forward(self):
            self.wait(self.got_far, self.landed.at[pl.ds(0, 2)])
            for side, step in ((0, 1), (1, -1)):
                total = self.sums[1 + side, rows_of(side), :].astype(F32) + self.landed[side].astype(F32)
                self.combined[side] = total.astype(BF16)
                self.send(self.combined.at[side], self.landed.at[4 + side], self.got, "x", step)

        def result(self, store):
            self.wait(self.got, self.landed.at[pl.ds(2, 4)])
            for side in (0, 1):
                store(
                    side,
                    self.own[3, rows_of(side), :]
                    + self.landed[3 - side].astype(F32)
                    + self.landed[4 + side].astype(F32),
                )


    def pair_up(sums, products):
        first, rest = products.groups

        def for_other(group):
            for i, j, value in products(group, 1 - core):
                sums[i].out[j] = value.astype(BF16)

        def for_this(group):
            for i, j, value in products(group, core):
                sums[i].own[j] = value

        def give(group):
            for j in group:
                for each in sums:
                    each.give(j)

        for_other(first)
        give(first)
        for_other(rest)
        for_this(first)
        give(rest)
        for each in sums:
            each.start()
        for_this(rest)

    r_mix = [Summed(fresh, t, out_0, in_0, sums_0, own_0, combined_0, landed_0) for t in streams]
    old = again(r_mix)
    r_one = [Summed(old, t, out_1, in_1, sums_1, own_1, combined_1, landed_1) for t in streams]
    r_two = [Summed(fresh, t, out_2, in_2, sums_2, own_2, combined_2, landed_2) for t in streams]

    def token_rows(t, side):
        return pl.ds(rows_each * t + half * side, half)

    reach = jnp.where(x == 0, 2, jnp.where(x == 1, 4, jnp.where(x == 2, 8, 16)))

    def mix():
        pooled = jnp.dot(scaled[...], mixer_in[...].reshape(2048, 128), preferred_element_type=F32)
        pooled = (pooled * rates[...]).astype(BF16)
        query = lax.broadcasted_iota(jnp.int32, (SEQ, SEQ), 0)
        earlier = lax.broadcasted_iota(jnp.int32, (SEQ, SEQ), 1)
        inside = jnp.where((earlier <= query) & (earlier > query - reach), 1.0, 0.0).astype(BF16)
        counts = jnp.minimum(query + 1, reach).astype(F32)
        scale = pool_s[...].astype(F32)
        sequences = [pooled[s * SEQ : s * SEQ + SEQ] for s in range(tokens // SEQ)]
        windows = [jnp.dot(inside, part, preferred_element_type=F32) for part in sequences]
        contrasts = [
            (window / counts - part.astype(F32)).astype(BF16) for window, part in zip(windows, sequences)
        ]
        mixed = jnp.dot(jnp.concatenate(contrasts, axis=0), pool_w[0], preferred_element_type=F32)
        group_out[...] = (mixed * scale).astype(BF16)

    def mix_products(group, owner_core):
        columns = []
        for j in group:
            pair = mixer_out[(x + Summed.steps[j]) % RING, pl.ds(2 * owner_core, 2)]
            columns.append(jnp.concatenate([pair[0], pair[1]], axis=1))
        for i, j in enumerate(group):
            both = jnp.dot(group_out[...], columns[i], preferred_element_type=F32)
            for t in streams:
                yield t, j, both[rows_each * t : rows_each * t + rows_each]

    mix_products.groups = ((0,), (1, 2, 3))

    def ffn_products(buf):
        def products(group, owner_core):
            columns = []
            for j in group:
                pair = buf[(x + Summed.steps[j]) % RING, pl.ds(2 * owner_core, 2)]
                early = jnp.concatenate([pair[0][:, :64], pair[1][:, :64]], axis=1)
                late = jnp.concatenate([pair[0][:, 64:], pair[1][:, 64:]], axis=1)
                columns.append(jnp.concatenate([early, late], axis=0))
            weights = jnp.concatenate(columns, axis=1)
            both = jnp.dot(hidden[...], weights, preferred_element_type=F32)
            for t in streams:
                for i, j in enumerate(group):
                    yield t, j, both[rows_each * t : rows_each * t + rows_each, 128 * i : 128 * i + 128]

        products.groups = ((0,), (1, 2, 3))
        return products

    def units(chunks):
        before = None
        for chunk in (*chunks, None):
            acts = None
            if chunk is not None:
                t, buf, at, width, column = chunk
                rows = slice(rows_each * t, rows_each * t + rows_each)
                weights = buf[:, :, :, at : at + 2 * width].reshape(2048, 2 * width)
                acts = jnp.dot(scaled[rows, :], weights, preferred_element_type=F32)
            if before is not None:
                done, (t, _, _, width, column) = before
                rows = slice(rows_each * t, rows_each * t + rows_each)
                rate = rates[rows, 0:width]
                gate, up = done[:, :width] * rate, done[:, width:] * rate
                hidden[rows, column : column + width] = (gate / (1.0 + jnp.exp(-gate)) * up).astype(BF16)
            before = acts, chunk

    def units_a(t):
        units([(t, pair_a, 256 * i, 128, 128 * i) for i in range(3)])

    def units_b(t):
        last = (t, pair_b, 512, 64, 640)
        units([*((t, pair_b, 256 * i, 128, 384 + 128 * i) for i in range(2)), last])

    def middle_of(t):
        def store(side, total):
            rows = token_rows(t, side)
            blocks_b[mine, rows, :] = (blocks_a[mine, rows, :].astype(F32) + total).astype(BF16)

        return store

    def first_of(t):
        def store(side, total):
            total_1[token_rows(t, side), :] = total

        return store

    def result_of(t):
        def store(side, second):
            rows = token_rows(t, side)
            first = total_1[rows, :]
            for i in (0, 1):
                lanes = slice(128 * i, 128 * i + 128)
                some = slice(64 * i, 64 * i + 64)
                total = jnp.concatenate([first[:, some], second[:, some]], axis=1)
                out[rows, lanes] = (blocks_b[mine, rows, lanes].astype(F32) + total).astype(BF16)

        return store

    def down_relay():
        g_da.p2_forward()
        g_db.p2_second()

    fetches[0].wait()
    s_in[0].start()
    fetches[1].wait()
    fetches[2].wait()
    g_in.p1_own()
    g_out.p1_own()
    s_in[1].start()
    fetches[3].wait()
    fetches[4].wait()
    for tile in range(5):
        buf, at = (pair_a, tile) if tile < 3 else (pair_b, tile - 3)
        some = slice(128 * tile, 128 * tile + 128)
        buf[z, y, :, 256 * at : 256 * at + 128] = gate_in[some, :].T
        buf[z, y, :, 256 * at + 128 : 256 * at + 256] = up_in[some, :].T
    pair_b[z, y, :, 512:640] = jnp.concatenate([gate_in[640:704, :], up_in[640:704, :]], axis=0).T
    for fetch in fetches[5:]:
        fetch.wait()
    for lane, buf in ((0, down_a), (64, down_b)):
        some = slice(lane, lane + 64)
        buf[z, y] = jnp.concatenate([down_in[0:352, some], down_in[352:704, some]], axis=1)
    mix_gain[...] = gains[0].astype(F32)
    ffn_gain[...] = gains[1].astype(F32)
    g_a.p1_own()
    g_b.p1_own()
    for t in streams:
        take(s_in[t], mix_gain, 0, first=True)
    g_in.p1_forward()
    g_out.p1_forward()
    g_da.p1_own()
    g_db.p1_own()
    s_in[0].forward()
    g_a.p1_forward()
    for t in streams:
        s_in[t].other_own()
        take(s_in[t], mix_gain, 0, other=True)
    s_in[0].near()
    s_in[1].forward()
    for step in (3, 1):
        take(s_in[0], mix_gain, step)
    g_in.p2_own()
    g_out.p2_own()
    g_b.p1_forward()
    s_in[1].near()
    for step in (3, 1):
        take(s_in[1], mix_gain, step)
    s_in[0].far()
    take(s_in[0], mix_gain, 2)
    s_in[1].far()
    take(s_in[1], mix_gain, 2)
    g_in.p2_forward()
    g_da.p1_forward()
    g_db.p1_forward()
    for t in streams:
        s_in[t].other_near()
        take(s_in[t], mix_gain, 3, other=True)
        take(s_in[t], mix_gain, 1, other=True)
        s_in[t].other_far()
        take(s_in[t], mix_gain, 2, other=True)
        row_rates(t)
    g_out.p2_forward()
    g_a.p2_own()
    g_in.finish()
    mix()
    g_out.finish()
    pair_up(r_mix, mix_products)
    r_mix[0].start_near()
    r_mix[1].start_near()
    g_b.p2_own()
    r_mix[0].forward()
    r_mix[1].forward()
    g_a.p2_forward()
    r_mix[0].result(middle_of(0))
    s_mid[0].start()
    take(s_mid[0], ffn_gain, 0, first=True)
    g_b.p2_forward()
    r_mix[1].result(middle_of(1))
    s_mid[1].start()
    take(s_mid[1], ffn_gain, 0, first=True)
    g_da.p2_own()
    g_db.p2_first()
    for t in streams:
        s_mid[t].other_own()
        take(s_mid[t], ffn_gain, 0, other=True)
    s_mid[0].forward()
    s_mid[0].near()
    s_mid[1].forward()
    for step in (3, 1):
        take(s_mid[0], ffn_gain, step)
    s_mid[1].near()
    s_mid[0].far()
    take(s_mid[0], ffn_gain, 2)
    for step in (3, 1):
        take(s_mid[1], ffn_gain, step)
    s_mid[1].far()
    take(s_mid[1], ffn_gain, 2)
    for t in streams:
        s_mid[t].other_near()
        take(s_mid[t], ffn_gain, 3, other=True)
        take(s_mid[t], ffn_gain, 1, other=True)
        s_mid[t].other_far()
        take(s_mid[t], ffn_gain, 2, other=True)
        row_rates(t)
    g_a.finish()
    units_a(0)
    down_relay()
    units_a(1)
    g_b.finish()
    units_b(0)
    units_b(1)
    g_db.p2_forward()
    g_da.finish()
    pair_up(r_one, ffn_products(down_a))
    for t in streams:
        r_one[t].start_near()
    g_db.finish()
    pair_up(r_two, ffn_products(down_b))
    for t in streams:
        r_one[t].forward()
    for t in streams:
        r_two[t].start_near()
    for t in streams:
        r_two[t].forward()
    for t in streams:
        r_one[t].result(first_of(t))
    for t in streams:
        r_two[t].result(result_of(t))

    pltpu.make_async_copy(tally, tally, sent).wait()


def summing(tokens, width):
    rows = tokens // 2
    return [
        pltpu.VMEM((2, 4, rows, width), BF16),
        pltpu.VMEM((2, 4, rows, width), BF16),
        pltpu.VMEM((2, 3, rows, width), BF16),
        pltpu.VMEM((2, 4, rows, width), F32),
        pltpu.VMEM((2, 2, rows // 2, width), BF16),
        pltpu.VMEM((2, 6, rows // 2, width), BF16),
    ]


def sent_rows(tokens):
    weights = 128 + 128 + 128 * 6 + 128 * 5 + 352 + 352
    return 15 * weights + 7 * tokens * 2 * (2 + 1) + 7 * tokens * 2


def on_device(stream, in_weight, pool_weight, pool_scale, out_weight, mix_gain, ffn_gain, gate_weight, up_weight, down_weight):
    tokens = stream.shape[0]
    return pl.pallas_call(
        kernel,
        out_shape=jax.ShapeDtypeStruct(stream.shape, BF16),
        in_specs=[pl.BlockSpec(memory_space=pltpu.HBM)] * 10,
        out_specs=pl.BlockSpec(memory_space=pltpu.VMEM),
        scratch_shapes=[
            pltpu.VMEM((2, 16, 128), BF16),
            pltpu.VMEM((16, 128), F32),
            pltpu.VMEM((16, 128), F32),
            pltpu.VMEM((704, 128), BF16),
            pltpu.VMEM((704, 128), BF16),
            pltpu.VMEM((704, 128), BF16),
            pltpu.VMEM((1, 128, 128), BF16),
            pltpu.VMEM((1, 128), BF16),
            pltpu.VMEM((4, 4, 128, 128), BF16),
            pltpu.VMEM((4, 4, 128, 128), BF16),
            pltpu.VMEM((4, 4, 128, 768), BF16),
            pltpu.VMEM((4, 4, 128, 640), BF16),
            pltpu.VMEM((4, 4, 352, 128), BF16),
            pltpu.VMEM((4, 4, 352, 128), BF16),
            pltpu.VMEM((8, tokens, 256), BF16),
            pltpu.VMEM((8, tokens, 256), BF16),
            pltpu.VMEM((tokens, 2048), BF16),
            pltpu.VMEM((tokens, 128), F32),
            pltpu.VMEM((tokens, 128), F32),
            pltpu.VMEM((tokens, 128), BF16),
            pltpu.VMEM((tokens, 704), BF16),
            *summing(tokens, 256),
            *summing(tokens, 128),
            pltpu.VMEM((tokens, 128), F32),
            *summing(tokens, 128),
            pltpu.VMEM((sent_rows(tokens), 128), BF16),
            pltpu.SemaphoreType.DMA((10,)),
            pltpu.SemaphoreType.DMA((53,)),
        ],
        compiler_params=pltpu.CompilerParams(
            collective_id=0, has_side_effects=True, vmem_limit_bytes=48 * 1024 * 1024
        ),
    )(*(pltpu.with_memory_space_constraint(a, pltpu.HBM) for a in (
        stream, in_weight, pool_weight, pool_scale.reshape(1, -1), out_weight,
        mix_gain.reshape(16, 128), ffn_gain.reshape(16, 128), gate_weight.T, up_weight.T, down_weight,
    )))


def solution(mesh):
    finer = Mesh(
        mesh.devices.reshape(mesh.shape["rep"], RING, RING, RING, 2),
        ("rep", "fs_0", "fs_1", "x", "core"),
    )
    fs, tp = ("fs_0", "fs_1"), ("x", "core")
    rows = ("rep", *fs)
    return jax.shard_map(
        on_device,
        mesh=finer,
        in_specs=(
            P(rows, tp), P(fs, tp), P(tp, None, None), P(tp), P(tp, fs),
            P(), P(), P(fs, tp), P(fs, tp), P(tp, fs),
        ),
        out_specs=P(rows, tp),
        check_vma=False,
    )
```

```python
import jax
import jax.numpy as jnp
from jax import lax
from jax.experimental import pallas as pl
from jax.experimental.pallas import tpu as pltpu
from jax.sharding import Mesh
from jax.sharding import PartitionSpec as P

SEQ = 128
RING = 4
EPS = 1e-06
F32, BF16 = jnp.float32, jnp.bfloat16


class Place:
    def __init__(self):
        self.rep, self.z, self.y = (lax.axis_index(a) for a in ("rep", "fs_0", "fs_1"))
        self.x, self.core = lax.axis_index("x"), lax.axis_index("core")

    def to(self, axis, step):
        if axis == "core":
            return {"core": 1 - self.core}
        if axis == "z":
            deep = (self.rep * RING + self.z + step + 2 * RING) % (2 * RING)
            return {"rep": deep // RING, "fs_0": deep % RING}
        index = {"x": self.x, "y": self.y}[axis]
        return {{"x": "x", "y": "fs_1"}[axis]: (index + step + RING) % RING}


class Net:
    def __init__(self, place, fresh, sent):
        self.place, self.fresh, self.sent = place, fresh, sent

    def send(self, src, dst, landed, axis, step):
        pltpu.make_async_remote_copy(
            src_ref=src,
            dst_ref=dst,
            send_sem=self.sent,
            recv_sem=landed,
            device_id=self.place.to(axis, step),
            device_id_type=pl.DeviceIdType.MESH,
        ).start()

    def wait(self, semaphore, as_many):
        pltpu.make_async_copy(as_many, as_many, semaphore).wait()


class Gather(Net):
    def __init__(self, place, fresh, sent, buf):
        super().__init__(place, fresh, sent)
        self.buf = buf
        half = buf.shape[2] // 2
        self.flows = (("y", "z", 0, half), ("z", "y", half, half))
        self.got_own, self.got_line, self.got_plane, self.got_all = (
            fresh() for _ in range(4)
        )

    def block(self, axis, step, first, rows):
        z, y = self.place.z, self.place.y
        z, y = ((z + step) % RING, y) if axis == "z" else (z, (y + step) % RING)
        return self.buf.at[z, y, pl.ds(first, rows), :]

    def plane(self, axis, step, side, first, rows):
        two = pl.ds(2 * side, 2)
        if axis == "z":
            return self.buf.at[(self.place.z + step) % RING, two, pl.ds(first, rows), :]
        return self.buf.at[two, (self.place.y + step) % RING, pl.ds(first, rows), :]

    def relay(self, part, landed, axis, step):
        self.send(part, part, landed, axis, step)

    def p1_own(self):
        for axis, _, first, rows in self.flows:
            own = self.block(axis, 0, first, rows)
            self.relay(own, self.got_own, axis, 1)
            self.relay(own, self.got_own, axis, -1)

    def p1_forward(self):
        self.wait(self.got_own, self.buf.at[0, pl.ds(0, 2)])
        for axis, _, first, rows in self.flows:
            half = (rows // 2 + 15) // 16 * 16
            self.relay(self.block(axis, 3, first, half), self.got_line, axis, 1)
            self.relay(self.block(axis, 1, first + half, rows - half), self.got_line, axis, -1)

    def p2_own(self):
        self.p2_first()
        self.p2_second()

    def p2_first(self):
        self.wait(self.got_line, self.buf.at[0, 0])
        for _, axis, first, rows in self.flows:
            low, high = (self.plane(axis, 0, side, first, rows) for side in (0, 1))
            self.relay(low, self.got_plane, axis, 1)
            self.relay(high, self.got_plane, axis, -1)

    def p2_second(self):
        for _, axis, first, rows in self.flows:
            low, high = (self.plane(axis, 0, side, first, rows) for side in (0, 1))
            self.relay(high, self.got_all, axis, 1)
            self.relay(low, self.got_all, axis, -1)

    def p2_forward(self):
        self.wait(self.got_plane, self.buf.at[0])
        for _, axis, first, rows in self.flows:
            self.relay(self.plane(axis, 3, 0, first, rows), self.got_all, axis, 1)
            self.relay(self.plane(axis, 1, 1, first, rows), self.got_all, axis, -1)

    def finish(self):
        self.wait(self.got_all, self.buf.at[pl.ds(0, 2)])


class Spread(Net):
    def __init__(self, place, fresh, sent, buf, first, rows):
        super().__init__(place, fresh, sent)
        self.buf, self.first, self.rows = buf, first, rows
        self.got_0, self.got_1, self.got_2, self.pair_0, self.pair_1, self.pair_2 = (
            fresh() for _ in range(6)
        )

    def index(self, step, other=False):
        core = 1 - self.place.core if other else self.place.core
        return 2 * ((self.place.x + step) % RING) + core

    def relay(self, step, side, landed, to):
        half = self.rows // 2
        part = self.buf.at[self.index(step), pl.ds(self.first + side * half, half), :]
        self.send(part, part, landed, "x", to)

    def to_core(self, step, landed):
        block = self.buf.at[self.index(step), pl.ds(self.first, self.rows), :]
        self.send(block, block, landed, "core", 0)

    def blocks(self, count):
        return self.buf.at[pl.ds(0, count), pl.ds(self.first, self.rows), :]

    def start(self):
        self.relay(0, 0, self.got_0, 1)
        self.relay(0, 1, self.got_0, -1)
        self.relay(0, 1, self.got_1, 1)
        self.relay(0, 0, self.got_1, -1)
        self.to_core(0, self.pair_0)

    def forward(self):
        self.wait(self.got_0, self.blocks(1))
        self.relay(3, 0, self.got_2, 1)
        self.relay(1, 1, self.got_2, -1)

    def near(self):
        self.wait(self.got_1, self.blocks(1))
        self.to_core(3, self.pair_1)
        self.to_core(1, self.pair_1)

    def far(self):
        self.wait(self.got_2, self.blocks(1))
        self.to_core(2, self.pair_2)

    def other_own(self):
        self.wait(self.pair_0, self.blocks(1))

    def other_near(self):
        self.wait(self.pair_1, self.blocks(2))

    def other_far(self):
        self.wait(self.pair_2, self.blocks(1))


def kernel(
    stream, w_in, pool_w_in, pool_s_in, w_out, mix_gain_in, ffn_gain_in, w_gate, w_up, w_down, out,
    gains, mix_gain, ffn_gain, gate_in, up_in, down_in, pool_w, pool_s,
    mixer_in, mixer_out, pair_a, pair_b, down_a, down_b, blocks_a, blocks_b, scaled, squares, rates, group_out, hidden,
    out_0, in_0, sums_0, own_0, combined_0, landed_0,
    out_1, in_1, sums_1, own_1, combined_1, landed_1, total_1,
    out_2, in_2, sums_2, own_2, combined_2, landed_2,
    tally, fetched, sems,
):
    place = Place()
    x, core, y, z = place.x, place.core, place.y, place.z
    mine = 2 * x + core
    tokens = stream.shape[0]

    barrier = pltpu.get_barrier_semaphore()
    neighbours = [place.to(a, s) for a in "xyz" for s in (1, -1)] + [place.to("core", 0)]
    fetches = [
        pltpu.make_async_copy(src, dst, fetched.at[i])
        for i, (src, dst) in enumerate((
            (stream, blocks_a.at[mine]),
            (w_in, mixer_in.at[z, y]),
            (w_out, mixer_out.at[z, y]),
            (w_gate, gate_in),
            (w_up, up_in),
            (w_down, down_in),
            (mix_gain_in, gains.at[0]),
            (ffn_gain_in, gains.at[1]),
            (pool_w_in, pool_w),
            (pool_s_in, pool_s),
        ))
    ]
    for i in (1, 2, 3, 4, 0, 5, 6, 7, 8, 9):
        fetches[i].start()
    for device in neighbours:
        pl.semaphore_signal(barrier, inc=1, device_id=device, device_id_type=pl.DeviceIdType.MESH)
    pl.semaphore_wait(barrier, len(neighbours))

    taken = iter(range(sems.shape[0]))

    def fresh():
        return sems.at[next(taken)]

    sent = fresh()
    gathers = [Gather(place, fresh, sent, buf) for buf in (mixer_in, mixer_out, pair_a, pair_b, down_a, down_b)]
    g_in, g_out, g_a, g_b, g_da, g_db = gathers
    streams = (0, 1)
    rows_each = tokens // 2
    half = rows_each // 2
    s_in = [Spread(place, fresh, sent, blocks_a, rows_each * t, rows_each) for t in streams]
    s_mid = [Spread(place, fresh, sent, blocks_b, rows_each * t, rows_each) for t in streams]

    def take(spread, gain_ref, step, other=False, first=False):
        index = spread.index(step, other)
        lanes = pl.ds(pl.multiple_of(index * 256, 256), 256)
        gain = jnp.concatenate([gain_ref[pl.ds(2 * index + i, 1), :] for i in (0, 1)], axis=1)

        def some(i, carry):
            rows = pl.ds(pl.multiple_of(spread.first + i * 64, 64), 64)
            value = spread.buf[index, rows, :].astype(F32)
            scaled[rows, lanes] = (value * gain).astype(BF16)
            square = value * value
            square = square[:, :128] + square[:, 128:]
            squares[rows, :] = square if first else squares[rows, :] + square
            return carry

        lax.fori_loop(0, spread.rows // 64, some, 0)

    def row_rates(t):
        rows = slice(rows_each * t, rows_each * t + rows_each)
        total = jnp.sum(squares[rows, :], axis=1, keepdims=True)
        rates[rows, :] = jnp.broadcast_to(lax.rsqrt(total * (1.0 / 2048.0) + EPS), (rows_each, 128))

    def rows_of(side):
        return pl.ds(side * half, half)

    class Summed(Net):
        steps = (2, 1, 3, 0)

        def __init__(self, t, *buffers):
            super().__init__(place, fresh, sent)
            self.out, self.into, self.sums, self.own, self.combined, self.landed = (
                buffer.at[t] for buffer in buffers
            )
            self.pair_0, self.pair_1, self.got_far, self.got = (
                fresh() for _ in range(4)
            )

        def give(self, j):
            landed = self.pair_1 if j else self.pair_0
            self.send(self.out.at[j], self.into.at[j], landed, "core", 0)

        def add(self, j):
            if j == 0:
                self.wait(self.pair_0, self.into.at[0])
            if j == 1:
                self.wait(self.pair_1, self.into.at[pl.ds(1, 3)])
            total = self.own[j] + self.into[j].astype(F32)
            if j == 3:
                self.own[j] = total
            else:
                self.sums[j] = total.astype(BF16)

        def start(self):
            sums, landed = self.sums, self.landed
            self.add(0)
            self.send(sums.at[0, rows_of(0)], landed.at[0], self.got_far, "x", 1)
            self.send(sums.at[0, rows_of(1)], landed.at[1], self.got_far, "x", -1)

        def start_near(self):
            sums, landed = self.sums, self.landed
            self.add(1)
            self.send(sums.at[1, rows_of(1)], landed.at[2], self.got, "x", 1)
            self.add(2)
            self.send(sums.at[2, rows_of(0)], landed.at[3], self.got, "x", -1)
            self.add(3)

        def forward(self):
            self.wait(self.got_far, self.landed.at[pl.ds(0, 2)])
            for side, step in ((0, 1), (1, -1)):
                total = self.sums[1 + side, rows_of(side), :].astype(F32) + self.landed[side].astype(F32)
                self.combined[side] = total.astype(BF16)
                self.send(self.combined.at[side], self.landed.at[4 + side], self.got, "x", step)

        def result(self, store):
            self.wait(self.got, self.landed.at[pl.ds(2, 4)])
            for side in (0, 1):
                store(
                    side,
                    self.own[3, rows_of(side), :]
                    + self.landed[3 - side].astype(F32)
                    + self.landed[4 + side].astype(F32),
                )


    def pair_up(sums, products):
        first, rest = products.groups

        def for_other(group):
            for i, j, value in products(group, 1 - core):
                sums[i].out[j] = value.astype(BF16)

        def for_this(group):
            for i, j, value in products(group, core):
                sums[i].own[j] = value

        def give(group):
            for j in group:
                for each in sums:
                    each.give(j)

        for_other(first)
        give(first)
        for_other(rest)
        for_this(first)
        give(rest)
        for each in sums:
            each.start()
        for_this(rest)

    r_mix = [Summed(t, out_0, in_0, sums_0, own_0, combined_0, landed_0) for t in streams]
    r_one = [Summed(t, out_1, in_1, sums_1, own_1, combined_1, landed_1) for t in streams]
    r_two = [Summed(t, out_2, in_2, sums_2, own_2, combined_2, landed_2) for t in streams]

    def token_rows(t, side):
        return pl.ds(rows_each * t + half * side, half)

    reach = jnp.where(x == 0, 2, jnp.where(x == 1, 4, jnp.where(x == 2, 8, 16)))

    def mix():
        pooled = jnp.dot(scaled[...], mixer_in[...].reshape(2048, 128), preferred_element_type=F32)
        pooled = (pooled * rates[...]).astype(BF16)
        query = lax.broadcasted_iota(jnp.int32, (SEQ, SEQ), 0)
        earlier = lax.broadcasted_iota(jnp.int32, (SEQ, SEQ), 1)
        inside = jnp.where((earlier <= query) & (earlier > query - reach), 1.0, 0.0).astype(BF16)
        counts = jnp.minimum(query + 1, reach).astype(F32)
        scale = pool_s[...].astype(F32)
        sequences = [pooled[s * SEQ : s * SEQ + SEQ] for s in range(tokens // SEQ)]
        windows = [jnp.dot(inside, part, preferred_element_type=F32) for part in sequences]
        contrasts = [
            (window / counts - part.astype(F32)).astype(BF16) for window, part in zip(windows, sequences)
        ]
        mixed = jnp.dot(jnp.concatenate(contrasts, axis=0), pool_w[0], preferred_element_type=F32)
        group_out[...] = (mixed * scale).astype(BF16)

    def mix_products(group, owner_core):
        columns = []
        for j in group:
            pair = mixer_out[(x + Summed.steps[j]) % RING, pl.ds(2 * owner_core, 2)]
            columns.append(jnp.concatenate([pair[0], pair[1]], axis=1))
        for i, j in enumerate(group):
            both = jnp.dot(group_out[...], columns[i], preferred_element_type=F32)
            for t in streams:
                yield t, j, both[rows_each * t : rows_each * t + rows_each]

    mix_products.groups = ((0,), (1, 2, 3))

    def ffn_products(buf):
        def products(group, owner_core):
            columns = []
            for j in group:
                pair = buf[(x + Summed.steps[j]) % RING, pl.ds(2 * owner_core, 2)]
                early = jnp.concatenate([pair[0][:, :64], pair[1][:, :64]], axis=1)
                late = jnp.concatenate([pair[0][:, 64:], pair[1][:, 64:]], axis=1)
                columns.append(jnp.concatenate([early, late], axis=0))
            weights = jnp.concatenate(columns, axis=1)
            both = jnp.dot(hidden[...], weights, preferred_element_type=F32)
            for t in streams:
                for i, j in enumerate(group):
                    yield t, j, both[rows_each * t : rows_each * t + rows_each, 128 * i : 128 * i + 128]

        products.groups = ((0,), (1, 2, 3))
        return products

    def units(chunks):
        before = None
        for chunk in (*chunks, None):
            acts = None
            if chunk is not None:
                t, buf, at, width, column = chunk
                rows = slice(rows_each * t, rows_each * t + rows_each)
                weights = buf[:, :, :, at : at + 2 * width].reshape(2048, 2 * width)
                acts = jnp.dot(scaled[rows, :], weights, preferred_element_type=F32)
            if before is not None:
                done, (t, _, _, width, column) = before
                rows = slice(rows_each * t, rows_each * t + rows_each)
                rate = rates[rows, 0:width]
                gate, up = done[:, :width] * rate, done[:, width:] * rate
                hidden[rows, column : column + width] = (gate / (1.0 + jnp.exp(-gate)) * up).astype(BF16)
            before = acts, chunk

    def units_a(t):
        units([(t, pair_a, 256 * i, 128, 128 * i) for i in range(3)])

    def units_b(t):
        last = (t, pair_b, 512, 64, 640)
        units([*((t, pair_b, 256 * i, 128, 384 + 128 * i) for i in range(2)), last])

    def middle_of(t):
        def store(side, total):
            rows = token_rows(t, side)
            blocks_b[mine, rows, :] = (blocks_a[mine, rows, :].astype(F32) + total).astype(BF16)

        return store

    def first_of(t):
        def store(side, total):
            total_1[token_rows(t, side), :] = total

        return store

    def result_of(t):
        def store(side, second):
            rows = token_rows(t, side)
            first = total_1[rows, :]
            for i in (0, 1):
                lanes = slice(128 * i, 128 * i + 128)
                some = slice(64 * i, 64 * i + 64)
                total = jnp.concatenate([first[:, some], second[:, some]], axis=1)
                out[rows, lanes] = (blocks_b[mine, rows, lanes].astype(F32) + total).astype(BF16)

        return store

    def down_relay():
        g_da.p2_forward()
        g_db.p2_second()

    fetches[1].wait()
    fetches[2].wait()
    g_in.p1_own()
    g_out.p1_own()
    fetches[0].wait()
    for t in streams:
        s_in[t].start()
    fetches[3].wait()
    fetches[4].wait()
    for tile in range(5):
        buf, at = (pair_a, tile) if tile < 3 else (pair_b, tile - 3)
        some = slice(128 * tile, 128 * tile + 128)
        buf[z, y, :, 256 * at : 256 * at + 128] = gate_in[some, :].T
        buf[z, y, :, 256 * at + 128 : 256 * at + 256] = up_in[some, :].T
    pair_b[z, y, :, 512:640] = jnp.concatenate([gate_in[640:704, :], up_in[640:704, :]], axis=0).T
    for fetch in fetches[5:]:
        fetch.wait()
    for lane, buf in ((0, down_a), (64, down_b)):
        some = slice(lane, lane + 64)
        buf[z, y] = jnp.concatenate([down_in[0:352, some], down_in[352:704, some]], axis=1)
    mix_gain[...] = gains[0].astype(F32)
    ffn_gain[...] = gains[1].astype(F32)
    g_a.p1_own()
    g_b.p1_own()
    for t in streams:
        take(s_in[t], mix_gain, 0, first=True)
    g_in.p1_forward()
    g_out.p1_forward()
    g_da.p1_own()
    g_db.p1_own()
    s_in[0].forward()
    g_a.p1_forward()
    for t in streams:
        s_in[t].other_own()
        take(s_in[t], mix_gain, 0, other=True)
    s_in[0].near()
    s_in[1].forward()
    for step in (3, 1):
        take(s_in[0], mix_gain, step)
    g_in.p2_own()
    g_out.p2_own()
    g_b.p1_forward()
    s_in[1].near()
    for step in (3, 1):
        take(s_in[1], mix_gain, step)
    s_in[0].far()
    take(s_in[0], mix_gain, 2)
    s_in[1].far()
    take(s_in[1], mix_gain, 2)
    g_in.p2_forward()
    g_da.p1_forward()
    g_db.p1_forward()
    for t in streams:
        s_in[t].other_near()
        take(s_in[t], mix_gain, 3, other=True)
        take(s_in[t], mix_gain, 1, other=True)
        s_in[t].other_far()
        take(s_in[t], mix_gain, 2, other=True)
        row_rates(t)
    g_out.p2_forward()
    g_a.p2_own()
    g_in.finish()
    mix()
    g_out.finish()
    pair_up(r_mix, mix_products)
    r_mix[0].start_near()
    r_mix[1].start_near()
    g_b.p2_own()
    r_mix[0].forward()
    r_mix[1].forward()
    g_a.p2_forward()
    r_mix[0].result(middle_of(0))
    s_mid[0].start()
    take(s_mid[0], ffn_gain, 0, first=True)
    g_b.p2_forward()
    r_mix[1].result(middle_of(1))
    s_mid[1].start()
    take(s_mid[1], ffn_gain, 0, first=True)
    g_da.p2_own()
    g_db.p2_first()
    for t in streams:
        s_mid[t].other_own()
        take(s_mid[t], ffn_gain, 0, other=True)
    s_mid[0].forward()
    s_mid[0].near()
    s_mid[1].forward()
    for step in (3, 1):
        take(s_mid[0], ffn_gain, step)
    s_mid[1].near()
    s_mid[0].far()
    take(s_mid[0], ffn_gain, 2)
    for step in (3, 1):
        take(s_mid[1], ffn_gain, step)
    s_mid[1].far()
    take(s_mid[1], ffn_gain, 2)
    for t in streams:
        s_mid[t].other_near()
        take(s_mid[t], ffn_gain, 3, other=True)
        take(s_mid[t], ffn_gain, 1, other=True)
        s_mid[t].other_far()
        take(s_mid[t], ffn_gain, 2, other=True)
        row_rates(t)
    g_a.finish()
    units_a(0)
    down_relay()
    units_a(1)
    g_b.finish()
    units_b(0)
    units_b(1)
    g_db.p2_forward()
    g_da.finish()
    pair_up(r_one, ffn_products(down_a))
    for t in streams:
        r_one[t].start_near()
    g_db.finish()
    pair_up(r_two, ffn_products(down_b))
    for t in streams:
        r_one[t].forward()
    for t in streams:
        r_two[t].start_near()
    for t in streams:
        r_two[t].forward()
    for t in streams:
        r_one[t].result(first_of(t))
    for t in streams:
        r_two[t].result(result_of(t))

    pltpu.make_async_copy(tally, tally, sent).wait()


def summing(tokens, width):
    rows = tokens // 2
    return [
        pltpu.VMEM((2, 4, rows, width), BF16),
        pltpu.VMEM((2, 4, rows, width), BF16),
        pltpu.VMEM((2, 3, rows, width), BF16),
        pltpu.VMEM((2, 4, rows, width), F32),
        pltpu.VMEM((2, 2, rows // 2, width), BF16),
        pltpu.VMEM((2, 6, rows // 2, width), BF16),
    ]


def sent_rows(tokens):
    weights = 128 + 128 + 128 * 6 + 128 * 5 + 352 + 352
    return 15 * weights + 7 * tokens * 2 * (2 + 1) + 7 * tokens * 2


def on_device(stream, in_weight, pool_weight, pool_scale, out_weight, mix_gain, ffn_gain, gate_weight, up_weight, down_weight):
    tokens = stream.shape[0]
    return pl.pallas_call(
        kernel,
        out_shape=jax.ShapeDtypeStruct(stream.shape, BF16),
        in_specs=[pl.BlockSpec(memory_space=pltpu.HBM)] * 10,
        out_specs=pl.BlockSpec(memory_space=pltpu.VMEM),
        scratch_shapes=[
            pltpu.VMEM((2, 16, 128), BF16),
            pltpu.VMEM((16, 128), F32),
            pltpu.VMEM((16, 128), F32),
            pltpu.VMEM((704, 128), BF16),
            pltpu.VMEM((704, 128), BF16),
            pltpu.VMEM((704, 128), BF16),
            pltpu.VMEM((1, 128, 128), BF16),
            pltpu.VMEM((1, 128), BF16),
            pltpu.VMEM((4, 4, 128, 128), BF16),
            pltpu.VMEM((4, 4, 128, 128), BF16),
            pltpu.VMEM((4, 4, 128, 768), BF16),
            pltpu.VMEM((4, 4, 128, 640), BF16),
            pltpu.VMEM((4, 4, 352, 128), BF16),
            pltpu.VMEM((4, 4, 352, 128), BF16),
            pltpu.VMEM((8, tokens, 256), BF16),
            pltpu.VMEM((8, tokens, 256), BF16),
            pltpu.VMEM((tokens, 2048), BF16),
            pltpu.VMEM((tokens, 128), F32),
            pltpu.VMEM((tokens, 128), F32),
            pltpu.VMEM((tokens, 128), BF16),
            pltpu.VMEM((tokens, 704), BF16),
            *summing(tokens, 256),
            *summing(tokens, 128),
            pltpu.VMEM((tokens, 128), F32),
            *summing(tokens, 128),
            pltpu.VMEM((sent_rows(tokens), 128), BF16),
            pltpu.SemaphoreType.DMA((10,)),
            pltpu.SemaphoreType.DMA((73,)),
        ],
        compiler_params=pltpu.CompilerParams(
            collective_id=0, has_side_effects=True, vmem_limit_bytes=48 * 1024 * 1024
        ),
    )(*(pltpu.with_memory_space_constraint(a, pltpu.HBM) for a in (
        stream, in_weight, pool_weight, pool_scale.reshape(1, -1), out_weight,
        mix_gain.reshape(16, 128), ffn_gain.reshape(16, 128), gate_weight.T, up_weight.T, down_weight,
    )))


def solution(mesh):
    finer = Mesh(
        mesh.devices.reshape(mesh.shape["rep"], RING, RING, RING, 2),
        ("rep", "fs_0", "fs_1", "x", "core"),
    )
    fs, tp = ("fs_0", "fs_1"), ("x", "core")
    rows = ("rep", *fs)
    return jax.shard_map(
        on_device,
        mesh=finer,
        in_specs=(
            P(rows, tp), P(fs, tp), P(tp, None, None), P(tp), P(tp, fs),
            P(), P(), P(fs, tp), P(fs, tp), P(tp, fs),
        ),
        out_specs=P(rows, tp),
        check_vma=False,
    )
```

```python
import jax
import jax.numpy as jnp
from jax import lax
from jax.experimental import pallas as pl
from jax.experimental.pallas import tpu as pltpu
from jax.sharding import Mesh
from jax.sharding import PartitionSpec as P

SEQ = 128
RING = 4
EPS = 1e-06
F32, BF16 = jnp.float32, jnp.bfloat16


class Place:
    def __init__(self):
        self.rep, self.z, self.y = (lax.axis_index(a) for a in ("rep", "fs_0", "fs_1"))
        self.x, self.core = lax.axis_index("x"), lax.axis_index("core")

    def to(self, axis, step):
        if axis == "core":
            return {"core": 1 - self.core}
        if axis == "z":
            deep = (self.rep * RING + self.z + step + 2 * RING) % (2 * RING)
            return {"rep": deep // RING, "fs_0": deep % RING}
        index = {"x": self.x, "y": self.y}[axis]
        return {{"x": "x", "y": "fs_1"}[axis]: (index + step + RING) % RING}


class Net:
    def __init__(self, place, fresh, sent):
        self.place, self.fresh, self.sent = place, fresh, sent

    def send(self, src, dst, landed, axis, step):
        pltpu.make_async_remote_copy(
            src_ref=src,
            dst_ref=dst,
            send_sem=self.sent,
            recv_sem=landed,
            device_id=self.place.to(axis, step),
            device_id_type=pl.DeviceIdType.MESH,
        ).start()

    def wait(self, semaphore, as_many):
        pltpu.make_async_copy(as_many, as_many, semaphore).wait()


class Gather(Net):
    def __init__(self, place, fresh, sent, buf):
        super().__init__(place, fresh, sent)
        self.buf = buf
        half = buf.shape[2] // 2
        self.flows = (("y", "z", 0, half), ("z", "y", half, half))
        self.got_own, self.got_line, self.got_plane, self.got_all = (
            fresh() for _ in range(4)
        )

    def block(self, axis, step, first, rows):
        z, y = self.place.z, self.place.y
        z, y = ((z + step) % RING, y) if axis == "z" else (z, (y + step) % RING)
        return self.buf.at[z, y, pl.ds(first, rows), :]

    def plane(self, axis, step, side, first, rows):
        two = pl.ds(2 * side, 2)
        if axis == "z":
            return self.buf.at[(self.place.z + step) % RING, two, pl.ds(first, rows), :]
        return self.buf.at[two, (self.place.y + step) % RING, pl.ds(first, rows), :]

    def relay(self, part, landed, axis, step):
        self.send(part, part, landed, axis, step)

    def p1_own(self):
        for axis, _, first, rows in self.flows:
            own = self.block(axis, 0, first, rows)
            self.relay(own, self.got_own, axis, 1)
            self.relay(own, self.got_own, axis, -1)

    def p1_forward(self):
        self.wait(self.got_own, self.buf.at[0, pl.ds(0, 2)])
        for axis, _, first, rows in self.flows:
            half = (rows // 2 + 15) // 16 * 16
            self.relay(self.block(axis, 3, first, half), self.got_line, axis, 1)
            self.relay(self.block(axis, 1, first + half, rows - half), self.got_line, axis, -1)

    def p2_own(self):
        self.p2_first()
        self.p2_second()

    def p2_first(self):
        self.wait(self.got_line, self.buf.at[0, 0])
        for _, axis, first, rows in self.flows:
            low, high = (self.plane(axis, 0, side, first, rows) for side in (0, 1))
            self.relay(low, self.got_plane, axis, 1)
            self.relay(high, self.got_plane, axis, -1)

    def p2_second(self):
        for _, axis, first, rows in self.flows:
            low, high = (self.plane(axis, 0, side, first, rows) for side in (0, 1))
            self.relay(high, self.got_all, axis, 1)
            self.relay(low, self.got_all, axis, -1)

    def p2_forward(self):
        self.wait(self.got_plane, self.buf.at[0])
        for _, axis, first, rows in self.flows:
            self.relay(self.plane(axis, 3, 0, first, rows), self.got_all, axis, 1)
            self.relay(self.plane(axis, 1, 1, first, rows), self.got_all, axis, -1)

    def finish(self):
        self.wait(self.got_all, self.buf.at[pl.ds(0, 2)])


class Spread(Net):
    def __init__(self, place, fresh, sent, buf, first, rows):
        super().__init__(place, fresh, sent)
        self.buf, self.first, self.rows = buf, first, rows
        self.got_0, self.got_1, self.got_2, self.pair_0, self.pair_1, self.pair_2 = (
            fresh() for _ in range(6)
        )

    def index(self, step, other=False):
        core = 1 - self.place.core if other else self.place.core
        return 2 * ((self.place.x + step) % RING) + core

    def relay(self, step, side, landed, to):
        half = self.rows // 2
        part = self.buf.at[self.index(step), pl.ds(self.first + side * half, half), :]
        self.send(part, part, landed, "x", to)

    def to_core(self, step, landed):
        block = self.buf.at[self.index(step), pl.ds(self.first, self.rows), :]
        self.send(block, block, landed, "core", 0)

    def blocks(self, count):
        return self.buf.at[pl.ds(0, count), pl.ds(self.first, self.rows), :]

    def start(self):
        self.relay(0, 0, self.got_0, 1)
        self.relay(0, 1, self.got_0, -1)
        self.relay(0, 1, self.got_1, 1)
        self.relay(0, 0, self.got_1, -1)
        self.to_core(0, self.pair_0)

    def forward(self):
        self.wait(self.got_0, self.blocks(1))
        self.relay(3, 0, self.got_2, 1)
        self.relay(1, 1, self.got_2, -1)

    def near(self):
        self.wait(self.got_1, self.blocks(1))
        self.to_core(3, self.pair_1)
        self.to_core(1, self.pair_1)

    def far(self):
        self.wait(self.got_2, self.blocks(1))
        self.to_core(2, self.pair_2)

    def other_own(self):
        self.wait(self.pair_0, self.blocks(1))

    def other_near(self):
        self.wait(self.pair_1, self.blocks(2))

    def other_far(self):
        self.wait(self.pair_2, self.blocks(1))


def kernel(
    stream, w_in, pool_w_in, pool_s_in, w_out, mix_gain_in, ffn_gain_in, w_gate, w_up, w_down, out,
    gains, mix_gain, ffn_gain, gate_in, up_in, down_in, pool_w, pool_s,
    mixer_in, mixer_out, pair_a, pair_b, down_a, down_b, blocks_a, blocks_b, scaled, squares, rates, group_out, hidden,
    out_0, in_0, sums_0, own_0, combined_0, landed_0,
    out_1, in_1, sums_1, own_1, combined_1, landed_1, total_1,
    out_2, in_2, sums_2, own_2, combined_2, landed_2,
    tally, fetched, sems,
):
    place = Place()
    x, core, y, z = place.x, place.core, place.y, place.z
    mine = 2 * x + core
    tokens = stream.shape[0]

    barrier = pltpu.get_barrier_semaphore()
    neighbours = [place.to(a, s) for a in "xyz" for s in (1, -1)] + [place.to("core", 0)]
    for device in neighbours:
        pl.semaphore_signal(barrier, inc=1, device_id=device, device_id_type=pl.DeviceIdType.MESH)
    fetches = [
        pltpu.make_async_copy(src, dst, fetched.at[i])
        for i, (src, dst) in enumerate((
            (stream, blocks_a.at[mine]),
            (w_in, mixer_in.at[z, y]),
            (w_out, mixer_out.at[z, y]),
            (w_gate, gate_in),
            (w_up, up_in),
            (w_down, down_in),
            (mix_gain_in, gains.at[0]),
            (ffn_gain_in, gains.at[1]),
            (pool_w_in, pool_w),
            (pool_s_in, pool_s),
        ))
    ]
    for fetch in fetches:
        fetch.start()
    pl.semaphore_wait(barrier, len(neighbours))

    taken = iter(range(sems.shape[0]))

    def fresh():
        return sems.at[next(taken)]

    sent = fresh()
    gathers = [Gather(place, fresh, sent, buf) for buf in (mixer_in, mixer_out, pair_a, pair_b, down_a, down_b)]
    g_in, g_out, g_a, g_b, g_da, g_db = gathers
    streams = (0, 1)
    rows_each = tokens // 2
    half = rows_each // 2
    s_in = [Spread(place, fresh, sent, blocks_a, rows_each * t, rows_each) for t in streams]
    s_mid = [Spread(place, fresh, sent, blocks_b, rows_each * t, rows_each) for t in streams]

    def take(spread, gain_ref, step, other=False, first=False):
        index = spread.index(step, other)
        lanes = pl.ds(pl.multiple_of(index * 256, 256), 256)
        gain = jnp.concatenate([gain_ref[pl.ds(2 * index + i, 1), :] for i in (0, 1)], axis=1)

        def some(i, carry):
            rows = pl.ds(pl.multiple_of(spread.first + i * 64, 64), 64)
            value = spread.buf[index, rows, :].astype(F32)
            scaled[rows, lanes] = (value * gain).astype(BF16)
            square = value * value
            square = square[:, :128] + square[:, 128:]
            squares[rows, :] = square if first else squares[rows, :] + square
            return carry

        lax.fori_loop(0, spread.rows // 64, some, 0)

    def row_rates(t):
        rows = slice(rows_each * t, rows_each * t + rows_each)
        total = jnp.sum(squares[rows, :], axis=1, keepdims=True)
        rates[rows, :] = jnp.broadcast_to(lax.rsqrt(total * (1.0 / 2048.0) + EPS), (rows_each, 128))

    def rows_of(side):
        return pl.ds(side * half, half)

    class Summed(Net):
        steps = (2, 1, 3, 0)

        def __init__(self, t, *buffers):
            super().__init__(place, fresh, sent)
            self.out, self.into, self.sums, self.own, self.combined, self.landed = (
                buffer.at[t] for buffer in buffers
            )
            self.pair_0, self.pair_1, self.got_far, self.got = (
                fresh() for _ in range(4)
            )

        def give(self, j):
            landed = self.pair_1 if j else self.pair_0
            self.send(self.out.at[j], self.into.at[j], landed, "core", 0)

        def add(self, j):
            if j == 0:
                self.wait(self.pair_0, self.into.at[0])
            if j == 1:
                self.wait(self.pair_1, self.into.at[pl.ds(1, 3)])
            total = self.own[j] + self.into[j].astype(F32)
            if j == 3:
                self.own[j] = total
            else:
                self.sums[j] = total.astype(BF16)

        def start(self):
            sums, landed = self.sums, self.landed
            self.add(0)
            self.send(sums.at[0, rows_of(0)], landed.at[0], self.got_far, "x", 1)
            self.send(sums.at[0, rows_of(1)], landed.at[1], self.got_far, "x", -1)

        def start_near(self):
            sums, landed = self.sums, self.landed
            self.add(1)
            self.send(sums.at[1, rows_of(1)], landed.at[2], self.got, "x", 1)
            self.add(2)
            self.send(sums.at[2, rows_of(0)], landed.at[3], self.got, "x", -1)
            self.add(3)

        def forward(self):
            self.wait(self.got_far, self.landed.at[pl.ds(0, 2)])
            for side, step in ((0, 1), (1, -1)):
                total = self.sums[1 + side, rows_of(side), :].astype(F32) + self.landed[side].astype(F32)
                self.combined[side] = total.astype(BF16)
                self.send(self.combined.at[side], self.landed.at[4 + side], self.got, "x", step)

        def result(self, store):
            self.wait(self.got, self.landed.at[pl.ds(2, 4)])
            for side in (0, 1):
                store(
                    side,
                    self.own[3, rows_of(side), :]
                    + self.landed[3 - side].astype(F32)
                    + self.landed[4 + side].astype(F32),
                )


    def pair_up(sums, products, earlier=()):
        first, rest = products.groups

        def for_other(group):
            for i, j, value in products(group, 1 - core):
                sums[i].out[j] = value.astype(BF16)

        def for_this(group):
            for i, j, value in products(group, core):
                sums[i].own[j] = value

        def give(group):
            for j in group:
                for each in sums:
                    each.give(j)

        for_other(first)
        give(first)
        for_other(rest)
        for_this(first)
        give(rest)
        for each in sums:
            each.start()
        for each in earlier:
            each.forward()
        for_this(rest)

    r_mix = [Summed(t, out_0, in_0, sums_0, own_0, combined_0, landed_0) for t in streams]
    r_one = [Summed(t, out_1, in_1, sums_1, own_1, combined_1, landed_1) for t in streams]
    r_two = [Summed(t, out_2, in_2, sums_2, own_2, combined_2, landed_2) for t in streams]

    def token_rows(t, side):
        return pl.ds(rows_each * t + half * side, half)

    reach = jnp.where(x == 0, 2, jnp.where(x == 1, 4, jnp.where(x == 2, 8, 16)))

    def mix():
        pooled = jnp.dot(scaled[...], mixer_in[...].reshape(2048, 128), preferred_element_type=F32)
        pooled = (pooled * rates[...]).astype(BF16)
        query = lax.broadcasted_iota(jnp.int32, (SEQ, SEQ), 0)
        earlier = lax.broadcasted_iota(jnp.int32, (SEQ, SEQ), 1)
        inside = jnp.where((earlier <= query) & (earlier > query - reach), 1.0, 0.0).astype(BF16)
        counts = jnp.minimum(query + 1, reach).astype(F32)
        scale = pool_s[...].astype(F32)
        sequences = [pooled[s * SEQ : s * SEQ + SEQ] for s in range(tokens // SEQ)]
        windows = [jnp.dot(inside, part, preferred_element_type=F32) for part in sequences]
        contrasts = [
            (window / counts - part.astype(F32)).astype(BF16) for window, part in zip(windows, sequences)
        ]
        mixed = jnp.dot(jnp.concatenate(contrasts, axis=0), pool_w[0], preferred_element_type=F32)
        group_out[...] = (mixed * scale).astype(BF16)

    def mix_products(group, owner_core):
        columns = []
        for j in group:
            pair = mixer_out[(x + Summed.steps[j]) % RING, pl.ds(2 * owner_core, 2)]
            columns.append(jnp.concatenate([pair[0], pair[1]], axis=1))
        for i, j in enumerate(group):
            both = jnp.dot(group_out[...], columns[i], preferred_element_type=F32)
            for t in streams:
                yield t, j, both[rows_each * t : rows_each * t + rows_each]

    mix_products.groups = ((0,), (1, 2, 3))

    def ffn_products(buf):
        def products(group, owner_core):
            columns = []
            for j in group:
                pair = buf[(x + Summed.steps[j]) % RING, pl.ds(2 * owner_core, 2)]
                early = jnp.concatenate([pair[0][:, :64], pair[1][:, :64]], axis=1)
                late = jnp.concatenate([pair[0][:, 64:], pair[1][:, 64:]], axis=1)
                columns.append(jnp.concatenate([early, late], axis=0))
            weights = jnp.concatenate(columns, axis=1)
            both = jnp.dot(hidden[...], weights, preferred_element_type=F32)
            for t in streams:
                for i, j in enumerate(group):
                    yield t, j, both[rows_each * t : rows_each * t + rows_each, 128 * i : 128 * i + 128]

        products.groups = ((0,), (1, 2, 3))
        return products

    def units(chunks):
        before = None
        for chunk in (*chunks, None):
            acts = None
            if chunk is not None:
                t, buf, at, width, column = chunk
                rows = slice(rows_each * t, rows_each * t + rows_each)
                weights = buf[:, :, :, at : at + 2 * width].reshape(2048, 2 * width)
                acts = jnp.dot(scaled[rows, :], weights, preferred_element_type=F32)
            if before is not None:
                done, (t, _, _, width, column) = before
                rows = slice(rows_each * t, rows_each * t + rows_each)
                rate = rates[rows, 0:width]
                gate, up = done[:, :width] * rate, done[:, width:] * rate
                hidden[rows, column : column + width] = (gate / (1.0 + jnp.exp(-gate)) * up).astype(BF16)
            before = acts, chunk

    def units_a(t):
        units([(t, pair_a, 256 * i, 128, 128 * i) for i in range(3)])

    def units_b(t):
        last = (t, pair_b, 512, 64, 640)
        units([*((t, pair_b, 256 * i, 128, 384 + 128 * i) for i in range(2)), last])

    def middle_of(t):
        def store(side, total):
            rows = token_rows(t, side)
            blocks_b[mine, rows, :] = (blocks_a[mine, rows, :].astype(F32) + total).astype(BF16)

        return store

    def first_of(t):
        def store(side, total):
            total_1[token_rows(t, side), :] = total

        return store

    def result_of(t):
        def store(side, second):
            rows = token_rows(t, side)
            first = total_1[rows, :]
            for i in (0, 1):
                lanes = slice(128 * i, 128 * i + 128)
                some = slice(64 * i, 64 * i + 64)
                total = jnp.concatenate([first[:, some], second[:, some]], axis=1)
                out[rows, lanes] = (blocks_b[mine, rows, lanes].astype(F32) + total).astype(BF16)

        return store

    def down_relay():
        g_da.p2_forward()
        g_db.p2_second()

    fetches[0].wait()
    s_in[0].start()
    fetches[1].wait()
    fetches[2].wait()
    g_in.p1_own()
    g_out.p1_own()
    s_in[1].start()
    fetches[3].wait()
    fetches[4].wait()
    for tile in range(5):
        buf, at = (pair_a, tile) if tile < 3 else (pair_b, tile - 3)
        some = slice(128 * tile, 128 * tile + 128)
        buf[z, y, :, 256 * at : 256 * at + 128] = gate_in[some, :].T
        buf[z, y, :, 256 * at + 128 : 256 * at + 256] = up_in[some, :].T
    pair_b[z, y, :, 512:640] = jnp.concatenate([gate_in[640:704, :], up_in[640:704, :]], axis=0).T
    for fetch in fetches[5:]:
        fetch.wait()
    for lane, buf in ((0, down_a), (64, down_b)):
        some = slice(lane, lane + 64)
        buf[z, y] = jnp.concatenate([down_in[0:352, some], down_in[352:704, some]], axis=1)
    mix_gain[...] = gains[0].astype(F32)
    ffn_gain[...] = gains[1].astype(F32)
    g_a.p1_own()
    g_b.p1_own()
    for t in streams:
        take(s_in[t], mix_gain, 0, first=True)
    g_in.p1_forward()
    g_out.p1_forward()
    g_da.p1_own()
    g_db.p1_own()
    s_in[0].forward()
    g_a.p1_forward()
    for t in streams:
        s_in[t].other_own()
        take(s_in[t], mix_gain, 0, other=True)
    s_in[0].near()
    s_in[1].forward()
    for step in (3, 1):
        take(s_in[0], mix_gain, step)
    g_in.p2_own()
    g_out.p2_own()
    g_b.p1_forward()
    s_in[1].near()
    for step in (3, 1):
        take(s_in[1], mix_gain, step)
    s_in[0].far()
    take(s_in[0], mix_gain, 2)
    s_in[1].far()
    take(s_in[1], mix_gain, 2)
    g_in.p2_forward()
    g_da.p1_forward()
    g_db.p1_forward()
    for t in streams:
        s_in[t].other_near()
        take(s_in[t], mix_gain, 3, other=True)
        take(s_in[t], mix_gain, 1, other=True)
        s_in[t].other_far()
        take(s_in[t], mix_gain, 2, other=True)
        row_rates(t)
    g_out.p2_forward()
    g_a.p2_own()
    g_in.finish()
    mix()
    g_out.finish()
    pair_up(r_mix, mix_products)
    r_mix[0].start_near()
    r_mix[1].start_near()
    g_b.p2_own()
    r_mix[0].forward()
    r_mix[1].forward()
    g_a.p2_forward()
    r_mix[0].result(middle_of(0))
    s_mid[0].start()
    take(s_mid[0], ffn_gain, 0, first=True)
    g_b.p2_forward()
    r_mix[1].result(middle_of(1))
    s_mid[1].start()
    take(s_mid[1], ffn_gain, 0, first=True)
    g_da.p2_own()
    g_db.p2_first()
    for t in streams:
        s_mid[t].other_own()
        take(s_mid[t], ffn_gain, 0, other=True)
    s_mid[0].forward()
    s_mid[0].near()
    s_mid[1].forward()
    for step in (3, 1):
        take(s_mid[0], ffn_gain, step)
    s_mid[1].near()
    s_mid[0].far()
    take(s_mid[0], ffn_gain, 2)
    for step in (3, 1):
        take(s_mid[1], ffn_gain, step)
    s_mid[1].far()
    take(s_mid[1], ffn_gain, 2)
    for t in streams:
        s_mid[t].other_near()
        take(s_mid[t], ffn_gain, 3, other=True)
        take(s_mid[t], ffn_gain, 1, other=True)
        s_mid[t].other_far()
        take(s_mid[t], ffn_gain, 2, other=True)
        row_rates(t)
    g_a.finish()
    units_a(0)
    down_relay()
    units_a(1)
    g_b.finish()
    units_b(0)
    units_b(1)
    g_db.p2_forward()
    g_da.finish()
    pair_up(r_one, ffn_products(down_a))
    for t in streams:
        r_one[t].start_near()
    g_db.finish()
    pair_up(r_two, ffn_products(down_b), r_one)
    for t in streams:
        r_two[t].start_near()
    for t in streams:
        r_two[t].forward()
    for t in streams:
        r_one[t].result(first_of(t))
    for t in streams:
        r_two[t].result(result_of(t))

    pltpu.make_async_copy(tally, tally, sent).wait()


def summing(tokens, width):
    rows = tokens // 2
    return [
        pltpu.VMEM((2, 4, rows, width), BF16),
        pltpu.VMEM((2, 4, rows, width), BF16),
        pltpu.VMEM((2, 3, rows, width), BF16),
        pltpu.VMEM((2, 4, rows, width), F32),
        pltpu.VMEM((2, 2, rows // 2, width), BF16),
        pltpu.VMEM((2, 6, rows // 2, width), BF16),
    ]


def sent_rows(tokens):
    weights = 128 + 128 + 128 * 6 + 128 * 5 + 352 + 352
    return 15 * weights + 7 * tokens * 2 * (2 + 1) + 7 * tokens * 2


def on_device(stream, in_weight, pool_weight, pool_scale, out_weight, mix_gain, ffn_gain, gate_weight, up_weight, down_weight):
    tokens = stream.shape[0]
    return pl.pallas_call(
        kernel,
        out_shape=jax.ShapeDtypeStruct(stream.shape, BF16),
        in_specs=[pl.BlockSpec(memory_space=pltpu.HBM)] * 10,
        out_specs=pl.BlockSpec(memory_space=pltpu.VMEM),
        scratch_shapes=[
            pltpu.VMEM((2, 16, 128), BF16),
            pltpu.VMEM((16, 128), F32),
            pltpu.VMEM((16, 128), F32),
            pltpu.VMEM((704, 128), BF16),
            pltpu.VMEM((704, 128), BF16),
            pltpu.VMEM((704, 128), BF16),
            pltpu.VMEM((1, 128, 128), BF16),
            pltpu.VMEM((1, 128), BF16),
            pltpu.VMEM((4, 4, 128, 128), BF16),
            pltpu.VMEM((4, 4, 128, 128), BF16),
            pltpu.VMEM((4, 4, 128, 768), BF16),
            pltpu.VMEM((4, 4, 128, 640), BF16),
            pltpu.VMEM((4, 4, 352, 128), BF16),
            pltpu.VMEM((4, 4, 352, 128), BF16),
            pltpu.VMEM((8, tokens, 256), BF16),
            pltpu.VMEM((8, tokens, 256), BF16),
            pltpu.VMEM((tokens, 2048), BF16),
            pltpu.VMEM((tokens, 128), F32),
            pltpu.VMEM((tokens, 128), F32),
            pltpu.VMEM((tokens, 128), BF16),
            pltpu.VMEM((tokens, 704), BF16),
            *summing(tokens, 256),
            *summing(tokens, 128),
            pltpu.VMEM((tokens, 128), F32),
            *summing(tokens, 128),
            pltpu.VMEM((sent_rows(tokens), 128), BF16),
            pltpu.SemaphoreType.DMA((10,)),
            pltpu.SemaphoreType.DMA((73,)),
        ],
        compiler_params=pltpu.CompilerParams(
            collective_id=0, has_side_effects=True, vmem_limit_bytes=48 * 1024 * 1024
        ),
    )(*(pltpu.with_memory_space_constraint(a, pltpu.HBM) for a in (
        stream, in_weight, pool_weight, pool_scale.reshape(1, -1), out_weight,
        mix_gain.reshape(16, 128), ffn_gain.reshape(16, 128), gate_weight.T, up_weight.T, down_weight,
    )))


def solution(mesh):
    finer = Mesh(
        mesh.devices.reshape(mesh.shape["rep"], RING, RING, RING, 2),
        ("rep", "fs_0", "fs_1", "x", "core"),
    )
    fs, tp = ("fs_0", "fs_1"), ("x", "core")
    rows = ("rep", *fs)
    return jax.shard_map(
        on_device,
        mesh=finer,
        in_specs=(
            P(rows, tp), P(fs, tp), P(tp, None, None), P(tp), P(tp, fs),
            P(), P(), P(fs, tp), P(fs, tp), P(tp, fs),
        ),
        out_specs=P(rows, tp),
        check_vma=False,
    )
```
